512 devices in a mesh: ep: 32 (over z, core), tp: 16 (over y, x).
Axes of the slice: x: 4, y: 4, z: 16, core: 2. Of those that a mesh axis runs over, the one named last changes fastest.
Arguments:
- tokens: bfloat16 [4096, 2048], P('ep'), may hold values from -6 to 6
- cotangent: bfloat16 [4096, 2048], P('ep'), may hold values from -6 to 6
- expert_ids: int32 [4096, 2], P('ep'), may hold values from 0 to 31, all different within a row; in each aligned block of 128 rows (0 to 127, 128 to 255, ...) at most 16 rows name the same one
- route_weight: bfloat16 [4096, 2], P('ep'), may hold values from 0.19921875 to 1
- gate_weight: bfloat16 [32, 1024, 2048], P('ep', 'tp'), may hold values from -0.125 to 0.125
- up_weight: bfloat16 [32, 1024, 2048], P('ep', 'tp'), may hold values from -0.125 to 0.125
- down_weight: bfloat16 [32, 1024, 2048], P('ep', 'tp'), may hold values from -0.1875 to 0.1875
Outputs:
- tokens_grad: bfloat16 [4096, 2048], P('ep', 'tp')
- route_weight_grad: float32 [4096, 2], P('ep')
- gate_weight_grad: float32 [32, 1024, 2048], P('ep', 'tp')
- up_weight_grad: float32 [32, 1024, 2048], P('ep', 'tp')
- down_weight_grad: float32 [32, 1024, 2048], P('ep', 'tp')
The draws below stay inside these ranges and needn't reach their ends.
Inputs may be any that keep to these rules, and one draw needn't show every extreme that they name: `expert_ids`: within each aligned block of 128 rows every expert is named at most 16 times; the two experts of a row differ.
All inputs are finite; a program needn't handle non-finite values.
Results may differ from the reference program's by a relative error of at most 0.0058.
Values may be sent and summed in bfloat16 or wider, within the bound.
A program may use at most 64 MiB of HBM per device.

```python
import math
import jax
import jax.numpy as jnp
import numpy as np
from jax import lax

D = 2048
FE = 1024
TOP = 2
TOK_DEV = 128
EXPERTS = 32
TOKENS = 4096
CAP = 16
N_EP = 32


def block_scale(rng, shape, split, smallest, high):
    loudness, own = 1.0, jax.random.fold_in(rng, 6)
    for axis_at, parts in split:
        draws = jnp.exp(jax.random.uniform(jax.random.fold_in(own, axis_at), (parts,), jnp.float32, smallest / len(split), high / len(split)))
        loudness = loudness * jnp.repeat(draws, shape[axis_at] // parts).reshape([-1 if axis == axis_at else 1 for axis in range(len(shape))])
    return loudness


def assign_block(own_key, own, number, rows, count, top, most, slope):
    sequence = jax.random.permutation(own_key, count)
    crowded, common = load_shares(count, rows * top, most, slope, True), load_shares(count, rows * top, most, slope, False)
    places = jnp.arange(count)

    def named(tallies, turn):
        used = int((tallies > 0).sum())
        fixed = max(1, used // 4)
        shifted = fixed + (places - fixed + turn * (used - fixed)) % max(1, count - fixed)
        return jnp.zeros((count,), jnp.int32).at[sequence[jnp.where(places < fixed, places, shifted)]].set(jnp.asarray(tallies, jnp.int32))

    tallies = jnp.where(number % 4 == 0, named(crowded, number // 4), named(common, number - number // 4 - 1))
    mixed = jax.random.permutation(jax.random.fold_in(own, 3), count)
    source_of, taker = mixed[0:count // 2 * 2:2], mixed[1:count // 2 * 2:2]
    slack = jnp.minimum(tallies[source_of] - 1, most - tallies[taker]) // 2
    slack = jnp.where((source_of == sequence[0]) | (taker == sequence[0]) | (tallies[taker] == 0), 0, jnp.maximum(slack, 0))
    shifted = jax.random.randint(jax.random.fold_in(own, 4), (count // 2,), 0, 1 << 20) % (slack + 1)
    tallies = tallies.at[source_of].add(-shifted).at[taker].add(shifted)
    items = jnp.searchsorted(jnp.cumsum(tallies), jnp.arange(rows * top), side="right").astype(jnp.int32)
    listing = items.reshape(top, rows).T
    listing = listing[jax.random.permutation(jax.random.fold_in(own, 1), rows)]
    turn = jax.random.randint(jax.random.fold_in(own, 2), (rows, 1), 0, top)
    return jnp.take_along_axis(listing, (jnp.arange(top)[None, :] + turn) % top, axis=1)


def load_shares(amount, total, most, slope, full):
    portions = [(1 << 20) // math.isqrt(rank ** slope) + 1 for rank in range(1, amount + 1)]
    largest = most if full else min(most, max(-(-total // amount), total * portions[0] // sum(portions)))
    least = 1 if total - largest >= amount - 1 else 0
    given, spare = [largest] + [least] * (amount - 1), total - largest - least * (amount - 1)
    while spare > 0:
        free = [i for i in range(1, amount) if given[i] < largest] or [i for i in range(1, amount) if given[i] < most]
        whole, left = sum([portions[i] for i in free]), spare
        for i in free:
            extra = min(most - given[i], max(1, left * portions[i] // whole), spare)
            given[i] = given[i] + extra
            spare = spare - extra
    return np.array(given)


def gaussian(stream_key, shape, spread, reach, cuts=(), kind=jnp.bfloat16):
    entries = spread * jax.random.normal(stream_key, shape, jnp.float32)
    if cuts:
        entries = entries * block_scale(stream_key, shape, cuts, -0.22, 0.18)
    return jnp.clip(entries, -reach, reach).astype(kind)


def setup_inputs(seed: int = 0) -> dict:
    streams_of = jax.random.split(jax.random.key(seed), 8)
    tokens = gaussian(streams_of[0], (TOKENS, D), 1.0, 6.0, ((0, 32),))
    cotangent = gaussian(streams_of[1], (TOKENS, D), 1.0, 6.0, ((0, 32),))
    expert_ids_keys = jax.random.split(jax.random.fold_in(streams_of[2], 1), TOKENS // TOK_DEV)
    expert_ids_turns = jax.random.permutation(jax.random.fold_in(streams_of[2], 3), TOKENS // TOK_DEV)
    expert_ids = jax.vmap(lambda own, number: assign_block(jax.random.fold_in(streams_of[2], 2), own, number, TOK_DEV, EXPERTS, TOP, CAP, 2))(expert_ids_keys, expert_ids_turns).reshape((TOKENS, TOP))
    route_weight = jnp.clip(0.19921875 + 0.80078125 * jax.random.uniform(streams_of[3], (TOKENS, TOP), jnp.float32) ** block_scale(streams_of[3], (TOKENS, TOP), ((0, 32),), -0.2, 0.2), 0.19921875, 1.0).astype(jnp.bfloat16)
    gate_weight = gaussian(streams_of[4], (EXPERTS, FE, D), D ** -0.5, 0.125, ((0, 32), (1, 16)))
    up_weight = gaussian(streams_of[5], (EXPERTS, FE, D), D ** -0.5, 0.125, ((0, 32), (1, 16)))
    down_weight = gaussian(streams_of[6], (EXPERTS, FE, D), FE ** -0.5, 0.1875, ((0, 32), (1, 16)))
    return {"tokens": tokens, "cotangent": cotangent, "expert_ids": expert_ids, "route_weight": route_weight, "gate_weight": gate_weight, "up_weight": up_weight, "down_weight": down_weight}


def reference(tokens, cotangent, expert_ids, route_weight, gate_weight, up_weight, down_weight):
    routed = TOKENS * TOP
    buffer_rows = N_EP * CAP
    flat_ids = expert_ids.reshape(-1)
    flat_weight = route_weight.reshape(-1)

    def one_expert(expert):
        picked = jnp.nonzero(flat_ids == expert, size=buffer_rows, fill_value=routed)[0].astype(jnp.int32)
        usable = picked < routed
        safe_pair = jnp.minimum(picked, routed - 1)
        token_of = safe_pair // TOP
        routed_rows = tokens[token_of]
        routed_cotangent = cotangent[token_of]
        weight = jnp.where(usable, flat_weight[safe_pair].astype(jnp.float32), jnp.float32(0.0))[:, None]
        gate_w = lax.dynamic_index_in_dim(gate_weight, expert, 0, keepdims=False)
        up_w = lax.dynamic_index_in_dim(up_weight, expert, 0, keepdims=False)
        down_w = lax.dynamic_index_in_dim(down_weight, expert, 0, keepdims=False)
        pre_gate = jnp.dot(routed_rows, gate_w.T, preferred_element_type=jnp.float32)
        pre_up = jnp.dot(routed_rows, up_w.T, preferred_element_type=jnp.float32)
        sigma = jax.nn.sigmoid(pre_gate)
        silu_gate = pre_gate * sigma
        hidden = silu_gate * pre_up
        back_hidden = jnp.dot(routed_cotangent, down_w.T, preferred_element_type=jnp.float32)
        products = jnp.sum(hidden * back_hidden, axis=1)
        scaled = weight * back_hidden
        grad_gate = (scaled * pre_up * sigma * (1.0 + pre_gate * (1.0 - sigma))).astype(jnp.bfloat16)
        grad_up = (scaled * silu_gate).astype(jnp.bfloat16)
        weighted = (weight * hidden).astype(jnp.bfloat16)
        down_grad = jnp.dot(weighted.T, routed_cotangent, preferred_element_type=jnp.float32)
        gate_grad = jnp.dot(grad_gate.T, routed_rows, preferred_element_type=jnp.float32)
        up_grad = jnp.dot(grad_up.T, routed_rows, preferred_element_type=jnp.float32)
        pair_grad = (jnp.dot(grad_gate, gate_w, preferred_element_type=jnp.float32)
                     + jnp.dot(grad_up, up_w, preferred_element_type=jnp.float32)).astype(jnp.bfloat16)
        return gate_grad, up_grad, down_grad, picked, pair_grad, products

    gate_grad, up_grad, down_grad, picked, pair_grad, products = lax.map(
        one_expert, jnp.arange(EXPERTS, dtype=jnp.int32))
    slot_flat = picked.reshape(-1)
    token_sum = jnp.zeros((routed, D), jnp.float32).at[slot_flat].set(
        pair_grad.reshape(-1, D).astype(jnp.float32), mode="drop")
    tokens_grad = jnp.sum(token_sum.reshape(TOKENS, TOP, D), axis=1).astype(jnp.bfloat16)
    route_grad = jnp.zeros((routed,), jnp.float32).at[slot_flat].set(products.reshape(-1), mode="drop")
    return tokens_grad, route_grad.reshape(TOKENS, TOP), gate_grad, up_grad, down_grad
```

```python
import functools

import jax
import jax.numpy as jnp
from jax import lax
from jax.experimental import pallas as pl
from jax.experimental.pallas import tpu as pltpu
from jax.sharding import PartitionSpec as P

MESH = pl.DeviceIdType.MESH
F32, BF16 = jnp.float32, jnp.bfloat16
CAP = 16
LANES = 128
CHUNKS = 4


def dot(a, b, dims=((1,), (0,))):
    return lax.dot_general(a, b, (dims, ((), ())), preferred_element_type=F32)


def kernel(nz, side, tok, cot, ids_ref, rw_ref, gw, uw, dw, tg_out, rg_out, gg_out, ug_out, dg_out,
           tokc, cotc, wgu, wd, send, rows, wx, wy, gsrc, grecv, ght, hht, pkeep, psrc, precv,
           pback, q0, q1r, q1s, q2r, qtot, ret, retq, ggv, ugv, dgv,
           sem_tc, sem_w, sem_wd, sem_out, s_a, r_a, s_b, r_b, s_w, r_w, s_g, r_g, s_p, r_p,
           s_q1, r_q1, s_q2, r_q2, s_e, r_e, s_f, r_f):
    n_ep, n_tp = 2 * nz, side * side
    slots = n_ep
    per = slots // CHUNKS
    sub = per // 2
    crows = per * CAP
    me, mt = lax.axis_index("ep"), lax.axis_index("tp")
    z, core = me // 2, lax.rem(me, 2)
    y, x = mt // side, lax.rem(mt, side)

    def at(dx, dy):
        return lax.rem(y + dy, side) * side + lax.rem(x + dx, side)

    def along(axis, d):
        return at(d, 0) if axis == 0 else at(0, d)

    def far(slot):
        i, rc = slot // 2, slot % 2
        d = (i + 1) // 2 if i % 2 else (nz - i // 2) % nz
        return lax.rem(z + d, nz) * 2 + lax.rem(core + rc, 2)

    def back_slot(slot):
        i, rc = slot // 2, slot % 2
        if 0 < i < nz - 1:
            i = i + 1 if i % 2 else i - 1
        return 2 * i + rc

    def rcopy(src, dst, ssem, rsem, ep, tp):
        return pltpu.make_async_remote_copy(
            src_ref=src, dst_ref=dst, send_sem=ssem, recv_sem=rsem,
            device_id={"ep": ep, "tp": tp}, device_id_type=MESH,
        )

    def got(ref, rsem):
        pltpu.make_async_copy(ref, ref, rsem).wait()

    barrier = pltpu.get_barrier_semaphore()

    def greet(i, carry):
        pl.semaphore_signal(barrier, inc=1, device_id={"ep": lax.rem(me + i, n_ep), "tp": mt}, device_id_type=MESH)
        return carry

    lax.fori_loop(1, n_ep, greet, 0)
    for d in range(1, side):
        for axis in range(2):
            pl.semaphore_signal(barrier, inc=1, device_id={"ep": me, "tp": along(axis, d)}, device_id_type=MESH)

    col = pl.ds(pl.multiple_of(mt * LANES, LANES), LANES)
    load_t = pltpu.make_async_copy(tok.at[:, col], tokc, sem_tc.at[0])
    load_c = pltpu.make_async_copy(cot.at[:, col], cotc, sem_tc.at[1])
    load_t.start()
    load_c.start()
    fh = gw.shape[1]

    for b in range(n_tp):
        cols = pl.ds(b * LANES, LANES)
        pltpu.make_async_copy(gw.at[0, :, cols], wgu.at[b, pl.ds(0, fh)], sem_w).start()
        pltpu.make_async_copy(uw.at[0, :, cols], wgu.at[b, pl.ds(fh, fh)], sem_w).start()
        for h in range(2):
            pltpu.make_async_copy(dw.at[0, :, cols], wd.at[b, pl.ds(h * fh, fh)], sem_wd).start()

    nt = tokc.shape[0]
    lane = lax.broadcasted_iota(jnp.int32, (nt, LANES), 1)
    row = lax.broadcasted_iota(jnp.int32, (nt, LANES), 0)
    ids = [ids_ref[:, k : k + 1] for k in range(2)]
    wt = [rw_ref[:, k : k + 1].astype(F32) for k in range(2)]
    mem = [(lane == ids[k]).astype(F32) for k in range(2)]
    lower = (lane < row).astype(BF16)
    before = dot(lower, (mem[0] + mem[1]).astype(BF16))
    rank = [jnp.sum(mem[k] * before, axis=1, keepdims=True).astype(jnp.int32) for k in range(2)]
    wide = lax.broadcasted_iota(jnp.int32, (nt, n_ep * CAP), 1)
    hot = [(wide == ids[k] * CAP + rank[k]).astype(F32) for k in range(2)]
    pick = hot[0] + hot[1]
    scaled = hot[0] * wt[0] + hot[1] * wt[1]
    pick_t = jnp.transpose(pick).astype(BF16)
    scaled_t = jnp.transpose(scaled).astype(BF16)
    load_t.wait()
    load_c.wait()
    send[:, 0] = dot(pick_t, tokc[...]).astype(BF16).reshape(n_ep, CAP, LANES)
    send[:, 1] = dot(scaled_t, cotc[...]).astype(BF16).reshape(n_ep, CAP, LANES)
    rows[mt, 0] = send[me]
    got(wgu, sem_w)
    got(wd, sem_wd)

    pl.semaphore_wait(barrier, n_ep - 1 + 2 * (side - 1))

    for s in range(1, slots):
        b = back_slot(s)
        e = far(s)
        rcopy(send.at[e], rows.at[mt, b], s_a, r_a.at[b // per], e, mt).start()
    for d in range(1, side):
        rcopy(wgu.reshape(side, side, LANES, LANES).at[:, lax.rem(x + d, side)], wx.at[side - d], s_w.at[0], r_w.at[0], me, along(0, d)).start()
        rcopy(wgu.reshape(side, side, LANES, LANES).at[lax.rem(y + d, side)], wy.at[side - d], s_w.at[1], r_w.at[1], me, along(1, d)).start()

    def place(axis, du, dv):
        return at(du, dv) if axis == 0 else at(dv, du)

    def pass_on(q, du, dv, second, step):
        axis = q % 2
        ref = rows.at[place(axis, du, dv), pl.ds(q * sub, sub)]
        rdu, rdv = (du, (dv - step) % side) if second else ((du - step) % side, dv)
        peer = along(1 - axis if second else axis, step % side)
        rcopy(ref, ref, s_b, r_b.at[(q * side + rdu) * side + rdv], me, peer).start()

    def block(q, du, dv):
        ref = rows.at[place(q % 2, du, dv), pl.ds(q * sub, sub)]
        got(ref, r_b.at[(q * side + du) * side + dv])

    def both(q, du, dv, second):
        pass_on(q, du, dv, second, 1)
        pass_on(q, du, dv, second, -1)

    def relay(q, keep, second):
        v = side - 1 if (q // 2) % 2 == 0 else 1
        step = 1 if v == side - 1 else -1
        pass_on(q, *((keep, v) if second else (v, keep)), second, step)

    def level0(g):
        if g == 0:
            got(rows.at[mt, pl.ds(1, per - 1)], r_a.at[0])
        else:
            got(rows.at[mt, pl.ds(g * per, per)], r_a.at[g])
        for q in (2 * g, 2 * g + 1):
            both(q, 0, 0, False)
            both(q, 0, 0, True)

    def second_in(q, du):
        block(q, du, 1)
        block(q, du, side - 1)
        relay(q, du, True)

    def level1(g):
        for q in (2 * g, 2 * g + 1):
            block(q, 1, 0)
            block(q, side - 1, 0)
            relay(q, 0, False)
            both(q, 1, 0, True)
            both(q, side - 1, 0, True)
        for q in (2 * g, 2 * g + 1):
            second_in(q, 0)

    def level2(g):
        for q in (2 * g, 2 * g + 1):
            block(q, 2, 0)
            both(q, 2, 0, True)
        for q in (2 * g, 2 * g + 1):
            second_in(q, 1)
            second_in(q, side - 1)

    def level3(g):
        for q in (2 * g, 2 * g + 1):
            second_in(q, 2)

    def level4(g):
        for q in (2 * g, 2 * g + 1):
            for du in range(side):
                block(q, du, 2)

    half = lax.broadcasted_iota(jnp.int32, (crows, LANES), 1) < fh

    def level5(g):
        pre = jnp.zeros((crows, LANES), F32)
        back = jnp.zeros((crows, LANES), F32)
        for b in range(0, n_tp, 2):
            a = [rows[b + i, pl.ds(g * per, per)] for i in range(2)]
            t = jnp.concatenate([a[i][:, 0].reshape(crows, LANES) for i in range(2)], axis=1)
            c = jnp.concatenate([a[i][:, 1].reshape(crows, LANES) for i in range(2)], axis=1)
            wt_b = jnp.concatenate([wgu[b], wgu[b + 1]], axis=1)
            wd_b = jnp.concatenate([wd[b], wd[b + 1]], axis=1)
            pre = pre + dot(t, wt_b, ((1,), (1,)))
            back = back + dot(c, wd_b, ((1,), (1,)))
        other = pltpu.roll(pre, fh, 1)
        gate = jnp.where(half, pre, other)
        up = jnp.where(half, other, pre)
        sig = jax.nn.sigmoid(gate)
        silu = gate * sig
        hidden = silu * up
        grad = back * jnp.where(half, up * sig * (1.0 + gate * (1.0 - sig)), silu)
        gsrc[g] = grad.astype(BF16)
        ght[:, g * crows : (g + 1) * crows] = jnp.transpose(grad).astype(BF16)
        hht[:, g * crows : (g + 1) * crows] = jnp.transpose(hidden)[:fh].astype(BF16)
        prod = jnp.transpose(jnp.where(half, hidden * back, 0.0))
        q0[g] = jnp.sum(prod, axis=0, keepdims=True)
        axis = g % 2
        for d in range(1, side):
            rcopy(gsrc.at[g], grecv.at[g, side - d], s_g, r_g.at[g], me, along(axis, d)).start()
        for d in range(1, side):
            rcopy(q0.at[g], q1r.at[g, side - d], s_q1, r_q1.at[g], me, along(0, d)).start()

    def level6(g):
        axis = g % 2
        if g < 2:
            got((wx if axis == 0 else wy).at[pl.ds(1, side - 1)], r_w.at[axis])
        got(grecv.at[g, pl.ds(1, side - 1)], r_g.at[g])
        wr = wx if axis == 0 else wy
        spot = y if axis == 0 else x
        lhs = [gsrc[g]] + [grecv[g, r] for r in range(1, side)]
        lhs = [jnp.concatenate(lhs[k : k + 2], axis=1) for k in range(0, side, 2)]
        for d in range(0, side, 2):
            acc = jnp.zeros((crows, 2 * LANES), F32)
            for k in range(0, side, 2):
                parts = []
                for r in (k, k + 1):
                    w = []
                    for dd in (d, d + 1):
                        w.append(wgu[along(1 - axis, dd)] if r == 0 else wr[r, lax.rem(spot + dd, side)])
                    parts.append(jnp.concatenate(w, axis=1))
                acc = acc + dot(lhs[k // 2], jnp.concatenate(parts, axis=0))
            for i, dd in enumerate((d, d + 1)):
                piece = acc[:, i * LANES : (i + 1) * LANES]
                if dd == 0:
                    pkeep[g] = piece
                else:
                    psrc[g, dd] = piece.astype(BF16)
        for d in range(1, side):
            rcopy(psrc.at[g, d], precv.at[g, side - d], s_p, r_p.at[g], me, along(1 - axis, d)).start()
        got(q1r.at[g, pl.ds(1, side - 1)], r_q1.at[g])
        q1s[g] = q0[g] + q1r[g, 1] + q1r[g, 2] + q1r[g, 3]
        for d in range(1, side):
            rcopy(q1s.at[g], q2r.at[g, side - d], s_q2, r_q2.at[g], me, along(1, d)).start()

    def level7(g):
        got(precv.at[g, pl.ds(1, side - 1)], r_p.at[g])
        total = pkeep[g]
        for r in range(1, side):
            total = total + precv[g, r].astype(F32)
        pback[g] = total.astype(BF16).reshape(per, CAP, LANES)
        got(q2r.at[g, pl.ds(1, side - 1)], r_q2.at[g])
        qtot[g] = q1s[g] + q2r[g, 1] + q2r[g, 2] + q2r[g, 3]
        for i in range(per):
            s = g * per + i
            if s == 0:
                ret[me] = pback[0, 0]
                retq[me] = qtot[0]
            else:
                e = far(s)
                rcopy(pback.at[g, i], ret.at[me], s_e, r_e, e, mt).start()
                rcopy(qtot.at[g], retq.at[me], s_f, r_f, e, mt).start()

    def weight_grads(which):
        outs = []
        for b in range(0, n_tp, 2):
            c = jnp.concatenate([rows[b + i, :, which].reshape(slots * CAP, LANES) for i in range(2)], axis=1)
            cols = slice(b * LANES, (b + 2) * LANES)
            if which == 0:
                r = dot(ght[...], c)
                ggv[0, :, cols] = r[:fh]
                ugv[0, :, cols] = r[fh:]
            else:
                dgv[0, :, cols] = dot(hht[...], c)
        pairs = ((ggv, gg_out, 0), (ugv, ug_out, 1)) if which == 0 else ((dgv, dg_out, 2),)
        for src, dst, k in pairs:
            copy = pltpu.make_async_copy(src, dst, sem_out.at[k])
            copy.start()
            outs.append(copy)
        return outs

    levels = [level0, level1, level2, level3, level4, level5, level6, level7]
    outs = []
    for t in range(CHUNKS + len(levels) - 1):
        for k in reversed(range(len(levels))):
            if 0 <= t - k < CHUNKS:
                levels[k](t - k)
        if t == CHUNKS + 4:
            outs += weight_grads(0)
        if t == CHUNKS + 6:
            outs += weight_grads(1)

    got(ret.at[pl.ds(0, n_ep - 1)], r_e)
    tg_out[...] = dot(pick.astype(BF16), ret[...].reshape(n_ep * CAP, LANES)).astype(BF16)
    got(retq.at[pl.ds(0, n_ep - 1)], r_f)
    cols = []
    for k in range(2):
        e_z, e_core = ids[k] // 2, lax.rem(ids[k], 2)
        d = lax.rem(z - e_z + nz, nz)
        i = jnp.where(d == 0, 0, jnp.where(d <= nz // 2, 2 * d - 1, 2 * (nz - d)))
        s = 2 * i + lax.rem(core + e_core, 2)
        want = lax.rem(s, per) * CAP + rank[k]
        acc = jnp.zeros((nt, LANES), F32)
        for e in range(n_ep):
            acc = jnp.where(ids[k] == e, retq[e], acc)
        acc = jnp.sum(jnp.where(lane == want, acc, 0.0), axis=1, keepdims=True)
        cols.append(acc / wt[k])
    rg_out[...] = jnp.concatenate(cols, axis=1)

    got(send.at[pl.ds(0, n_ep - 1)], s_a)
    got(rows.at[pl.ds(0, n_tp - 1)], s_b)
    got(wx.at[pl.ds(1, side - 1)], s_w.at[0])
    got(wy.at[pl.ds(1, side - 1)], s_w.at[1])
    got(grecv.at[:, pl.ds(1, side - 1)], s_g)
    got(precv.at[:, pl.ds(1, side - 1)], s_p)
    got(q1r.at[:, pl.ds(1, side - 1)], s_q1)
    got(q2r.at[:, pl.ds(1, side - 1)], s_q2)
    got(ret.at[pl.ds(0, n_ep - 1)], s_e)
    got(retq.at[pl.ds(0, n_ep - 1)], s_f)
    for copy in outs:
        copy.wait()


def per_device(nz, side, tokens, cotangent, expert_ids, route_weight, gate_weight, up_weight, down_weight):
    n_ep, n_tp = 2 * nz, side * side
    per = n_ep // CHUNKS
    crows = per * CAP
    nt, width = tokens.shape
    fh = gate_weight.shape[1]
    vmem = pl.BlockSpec(memory_space=pltpu.VMEM)
    hbm = pl.BlockSpec(memory_space=pl.ANY)
    wshape = jax.ShapeDtypeStruct(gate_weight.shape, F32)
    dma = pltpu.SemaphoreType.DMA
    scratch = [
        pltpu.VMEM((nt, LANES), BF16),
        pltpu.VMEM((nt, LANES), BF16),
        pltpu.VMEM((n_tp, LANES, LANES), BF16),
        pltpu.VMEM((n_tp, LANES, LANES), BF16),
        pltpu.VMEM((n_ep, 2, CAP, LANES), BF16),
        pltpu.VMEM((n_tp, n_ep, 2, CAP, LANES), BF16),
        pltpu.VMEM((side, side, LANES, LANES), BF16),
        pltpu.VMEM((side, side, LANES, LANES), BF16),
        pltpu.VMEM((CHUNKS, crows, LANES), BF16),
        pltpu.VMEM((CHUNKS, side, crows, LANES), BF16),
        pltpu.VMEM((LANES, n_ep * CAP), BF16),
        pltpu.VMEM((fh, n_ep * CAP), BF16),
        pltpu.VMEM((CHUNKS, crows, LANES), F32),
        pltpu.VMEM((CHUNKS, side, crows, LANES), BF16),
        pltpu.VMEM((CHUNKS, side, crows, LANES), BF16),
        pltpu.VMEM((CHUNKS, per, CAP, LANES), BF16),
        pltpu.VMEM((CHUNKS, 1, LANES), F32),
        pltpu.VMEM((CHUNKS, side, 1, LANES), F32),
        pltpu.VMEM((CHUNKS, 1, LANES), F32),
        pltpu.VMEM((CHUNKS, side, 1, LANES), F32),
        pltpu.VMEM((CHUNKS, 1, LANES), F32),
        pltpu.VMEM((n_ep, CAP, LANES), BF16),
        pltpu.VMEM((n_ep, 1, LANES), F32),
        pltpu.VMEM(gate_weight.shape, F32),
        pltpu.VMEM(gate_weight.shape, F32),
        pltpu.VMEM(gate_weight.shape, F32),
        dma((2,)), dma, dma, dma((3,)),
        dma, dma((CHUNKS,)),
        dma, dma((2 * CHUNKS * n_tp,)),
        dma((2,)), dma((2,)),
        dma, dma((CHUNKS,)),
        dma, dma((CHUNKS,)),
        dma, dma((CHUNKS,)),
        dma, dma((CHUNKS,)),
        dma, dma,
        dma, dma,
    ]
    return tuple(pl.pallas_call(
        functools.partial(kernel, nz, side),
        out_shape=(
            jax.ShapeDtypeStruct((nt, LANES), BF16),
            jax.ShapeDtypeStruct((nt, 2), F32),
            wshape, wshape, wshape,
        ),
        in_specs=[hbm, hbm, vmem, vmem, hbm, hbm, hbm],
        out_specs=(vmem, vmem, hbm, hbm, hbm),
        scratch_shapes=scratch,
        compiler_params=pltpu.CompilerParams(collective_id=0, has_side_effects=True, vmem_limit_bytes=48 * 1024 * 1024),
    )(tokens, cotangent, expert_ids, route_weight, gate_weight, up_weight, down_weight))


def solution(mesh):
    nz = mesh.shape["ep"] // 2
    side = 4
    in_specs = (
        P("ep", None), P("ep", None), P("ep", None), P("ep", None),
        P("ep", "tp", None), P("ep", "tp", None), P("ep", "tp", None),
    )
    out_specs = (
        P("ep", "tp"), P("ep", None), P("ep", "tp", None), P("ep", "tp", None), P("ep", "tp", None),
    )
    return jax.shard_map(
        functools.partial(per_device, nz, side), mesh=mesh, in_specs=in_specs, out_specs=out_specs, check_vma=False
    )
```

```python
import functools

import jax
import jax.numpy as jnp
from jax import lax
from jax.experimental import pallas as pl
from jax.experimental.pallas import tpu as pltpu
from jax.sharding import PartitionSpec as P

MESH = pl.DeviceIdType.MESH
F32, BF16 = jnp.float32, jnp.bfloat16
CAP = 16
LANES = 128
SIZES = (8, 8, 8, 8)
CHUNKS = len(SIZES)
START = tuple(sum(SIZES[:g]) for g in range(CHUNKS))
SIDE = 4


def dot(a, b, dims=((1,), (0,)), **kw):
    return lax.dot_general(a, b, (dims, ((), ())), preferred_element_type=F32, **kw)


def slot_order(nz):
    near = [0] + [d for k in range(1, nz // 2) for d in (k, nz - k)] + [nz // 2]
    n = nz // 4
    return near[:n] + near[2 * n :] + near[n : 2 * n]


FIRST_AXIS = (0, 1) * CHUNKS
FIRST_STEP = (1, 1, -1, -1) * CHUNKS
DIRECT1 = tuple(range(2 * CHUNKS))
DIRECT2 = ()
WEIGHTS_AT = -1
AHEAD = 0


def kernel(nz, tok, cot, ids_hbm, rw_hbm, gw, uw, dw, tg_out, rg_out, gg_out, ug_out, dg_out,
           ids_ref, rw_ref, tokc, cotc, wgu, wd, send, rows, wx, gsrc, hsrc, grecv, pkeep, psrc, precv,
           pback, q0, q1r, q1s, q2r, qsend, ret, retq, pickv,
           sem_i, sem_tc, sem_w, sem_wd, s_a, r_a, s_b, r_b, s_w, r_w, s_g, r_g, s_p, r_p,
           s_q1, r_q1, s_q2, r_q2, s_e, r_e, s_f, r_f):
    side = SIDE
    n_ep, n_tp = 2 * nz, side * side
    order = slot_order(nz)
    slots = n_ep
    own = 2 * order.index(0)
    assert own == 0 and sum(SIZES) == slots
    me, mt = lax.axis_index("ep"), lax.axis_index("tp")
    z, core = me // 2, lax.rem(me, 2)
    y, x = mt // side, lax.rem(mt, side)
    fh = gw.shape[1]
    nt = tokc.shape[0]

    col = pl.ds(pl.multiple_of(mt * LANES, LANES), LANES)
    load_i = pltpu.make_async_copy(ids_hbm, ids_ref, sem_i.at[0])
    load_r = pltpu.make_async_copy(rw_hbm, rw_ref, sem_i.at[1])
    load_t = pltpu.make_async_copy(tok.at[:, col], tokc, sem_tc.at[0])
    load_c = pltpu.make_async_copy(cot.at[:, col], cotc, sem_tc.at[1])
    for load in (load_i, load_r, load_t, load_c):
        load.start()

    def at(dx, dy):
        return lax.rem(y + dy, side) * side + lax.rem(x + dx, side)

    def along(axis, d):
        return at(d, 0) if axis == 0 else at(0, d)

    def far(slot):
        return lax.rem(z + order[slot // 2], nz) * 2 + lax.rem(core + slot % 2, 2)

    def back_slot(slot):
        return 2 * order.index((nz - order[slot // 2]) % nz) + slot % 2

    def rcopy(src, dst, ssem, rsem, ep, tp):
        return pltpu.make_async_remote_copy(
            src_ref=src, dst_ref=dst, send_sem=ssem, recv_sem=rsem,
            device_id={"ep": ep, "tp": tp}, device_id_type=MESH,
        )

    def got(ref, rsem):
        pltpu.make_async_copy(ref, ref, rsem).wait()

    barrier = pltpu.get_barrier_semaphore()

    def greet(i, carry):
        pl.semaphore_signal(barrier, inc=1, device_id={"ep": lax.rem(me + i, n_ep), "tp": mt}, device_id_type=MESH)
        return carry

    lax.fori_loop(1, n_ep, greet, 0)
    for d in range(1, side):
        for axis in range(2):
            pl.semaphore_signal(barrier, inc=1, device_id={"ep": me, "tp": along(axis, d)}, device_id_type=MESH)

    for b in range(n_tp):
        cols = pl.ds(b * LANES, LANES)
        pltpu.make_async_copy(gw.at[0, :, cols], wgu.at[b, pl.ds(0, fh)], sem_w).start()
        pltpu.make_async_copy(uw.at[0, :, cols], wgu.at[b, pl.ds(fh, fh)], sem_w).start()

    load_i.wait()
    load_r.wait()
    ids = [ids_ref[k : k + 1, :] for k in range(2)]
    wt = [rw_ref[k : k + 1, :].astype(F32) for k in range(2)]
    e_row = lax.broadcasted_iota(jnp.int32, (n_ep, nt), 0)
    mem = [(e_row == ids[k]).astype(F32) for k in range(2)]
    upper = (lax.broadcasted_iota(jnp.int32, (nt, nt), 0) < lax.broadcasted_iota(jnp.int32, (nt, nt), 1)).astype(BF16)
    before = dot((mem[0] + mem[1]).astype(BF16), upper)
    rank = [jnp.sum(mem[k] * before, axis=0, keepdims=True).astype(jnp.int32) for k in range(2)]
    place_of = [ids[k] * CAP + rank[k] for k in range(2)]

    def hot(k):
        return (lax.broadcasted_iota(jnp.int32, (n_ep * CAP, nt), 0) == place_of[k]).astype(F32)

    h0, h1 = hot(0), hot(1)
    pick_t = h0 + h1
    scaled_t = h0 * wt[0] + h1 * wt[1]
    load_t.wait()
    load_c.wait()
    send[:, 0] = dot(pick_t.astype(BF16), tokc[...]).astype(BF16).reshape(n_ep, CAP, LANES)
    send[:, 1] = dot(scaled_t.astype(BF16), cotc[...]).astype(BF16).reshape(n_ep, CAP, LANES)
    rows[mt, own] = send[me]
    got(wgu, sem_w)

    with jax.named_scope("bar"):
        pl.semaphore_wait(barrier, n_ep - 1 + 2 * (side - 1))

    def dispatch(chunk):
        for s in range(START[chunk], START[chunk] + SIZES[chunk]):
            if s != own:
                e = far(back_slot(s))
                rcopy(send.at[e], rows.at[mt, s], s_a, r_a.at[chunk], e, mt).start()

    dispatch(0)

    def weights_out():
        w4 = wgu.reshape(side, side, LANES, LANES)
        for d in range(1, side):
            rcopy(w4.at[:, lax.rem(x + d, side)], wx.at[side - d], s_w, r_w, me, along(0, d)).start()

    if WEIGHTS_AT < 0:
        weights_out()
    for b in range(n_tp):
        cols = pl.ds(b * LANES, LANES)
        for h in range(2):
            pltpu.make_async_copy(dw.at[0, :, cols], wd.at[b, pl.ds(h * fh, fh)], sem_wd).start()
    pickv[...] = jnp.transpose(pick_t).astype(BF16)
    got(wd, sem_wd)
    for chunk in range(1, CHUNKS):
        dispatch(chunk)

    def ref_of(q, du, dv):
        b = at(du, dv) if FIRST_AXIS[q] == 0 else at(dv, du)
        g, n = q // 2, SIZES[q // 2] // 2
        return rows.at[b, pl.ds(START[g] + q % 2 * n, n)]

    def span(g):
        return pl.ds(START[g] * CAP, SIZES[g] * CAP)

    def pass_on(q, du, dv, second, step):
        rdu, rdv = (du, (dv - step) % side) if second else ((du - step) % side, dv)
        axis = FIRST_AXIS[q] ^ int(second)
        ref = ref_of(q, du, dv)
        rcopy(ref, ref, s_b, r_b.at[(q * side + rdu) * side + rdv], me, along(axis, step % side)).start()

    def block(q, du, dv):
        got(ref_of(q, du, dv), r_b.at[(q * side + du) * side + dv])

    def both(q, du, dv, second):
        pass_on(q, du, dv, second, 1)
        pass_on(q, du, dv, second, -1)

    def relay(q, keep, second):
        step = FIRST_STEP[q] if not second else 1 if (q + keep) % 2 == 0 else -1
        v = side - 1 if step == 1 else 1
        pass_on(q, *((keep, v) if second else (v, keep)), second, step)

    def spread(q, du):
        both(q, du, 0, True)
        if q in DIRECT2:
            pass_on(q, du, 0, True, 2)

    def halves(g):
        return (2 * g, 2 * g + 1)

    def level0(g):
        skip = 1 if g == 0 else 0
        got(rows.at[mt, pl.ds(START[g] + skip, SIZES[g] - skip)], r_a.at[g])
        for q in halves(g):
            both(q, 0, 0, False)
            if q in DIRECT1:
                pass_on(q, 0, 0, False, 2)
        for q in halves(g):
            spread(q, 0)
        if g == WEIGHTS_AT:
            weights_out()

    def second_in(q, du):
        if q not in DIRECT2:
            block(q, du, 1)
            block(q, du, side - 1)
            relay(q, du, True)

    def level1(g):
        for q in halves(g):
            block(q, 1, 0)
            block(q, side - 1, 0)
            if q not in DIRECT1:
                relay(q, 0, False)
            spread(q, 1)
            spread(q, side - 1)
        for q in halves(g):
            second_in(q, 0)

    def level2(g):
        for q in halves(g):
            block(q, 2, 0)
            spread(q, 2)
        for q in halves(g):
            second_in(q, 1)
            second_in(q, side - 1)

    def level3(g):
        for q in halves(g):
            second_in(q, 2)

    def level4(g):
        for q in halves(g):
            for du in range(side):
                if q in DIRECT2:
                    block(q, du, 1)
                    block(q, du, side - 1)
                block(q, du, 2)

    def level5(g):
        per = SIZES[g]
        crows = per * CAP
        half = lax.broadcasted_iota(jnp.int32, (crows, LANES), 1) < fh
        pre = jnp.zeros((crows, LANES), F32)
        back = jnp.zeros((crows, LANES), F32)
        for b in range(0, n_tp, 2):
            a = [rows[b + i, pl.ds(START[g], per)] for i in range(2)]
            t = jnp.concatenate([a[i][:, 0].reshape(crows, LANES) for i in range(2)], axis=1)
            c = jnp.concatenate([a[i][:, 1].reshape(crows, LANES) for i in range(2)], axis=1)
            wt_b = jnp.concatenate([wgu[b], wgu[b + 1]], axis=1)
            wd_b = jnp.concatenate([wd[b], wd[b + 1]], axis=1)
            pre = pre + dot(t, wt_b, ((1,), (1,)))
            back = back + dot(c, wd_b, ((1,), (1,)))
        other = pltpu.roll(pre, fh, 1)
        gate = jnp.where(half, pre, other)
        up = jnp.where(half, other, pre)
        sig = jax.nn.sigmoid(gate)
        silu = gate * sig
        hidden = silu * up
        grad = back * jnp.where(half, up * sig * (1.0 + gate * (1.0 - sig)), silu)
        gsrc[span(g)] = grad.astype(BF16)
        hsrc[span(g)] = hidden.astype(BF16)
        prod = jnp.where(half, hidden * back, 0.0)
        if crows < LANES:
            prod = jnp.concatenate([prod, jnp.zeros((LANES - crows, LANES), F32)], axis=0)
        prod = jnp.transpose(prod)
        q0[g] = jnp.sum(prod, axis=0, keepdims=True)
        for d in range(1, side):
            rcopy(gsrc.at[span(g)], grecv.at[side - d, span(g)], s_g, r_g.at[g], me, along(0, d)).start()
        for d in range(1, side):
            rcopy(q0.at[g], q1r.at[g, side - d], s_q1, r_q1.at[g], me, along(0, d)).start()

    def level6(g):
        if g == 0:
            got(wx.at[pl.ds(1, side - 1)], r_w)
        crows = SIZES[g] * CAP
        got(grecv.at[pl.ds(1, side - 1), span(g)], r_g.at[g])
        lhs = [gsrc[span(g)]] + [grecv[r, span(g)] for r in range(1, side)]
        lhs = [jnp.concatenate(lhs[k : k + 2], axis=1) for k in range(0, side, 2)]
        for d in reversed(range(0, side, 2)):
            acc = jnp.zeros((crows, 2 * LANES), F32)
            for k in range(0, side, 2):
                parts = []
                for r in (k, k + 1):
                    w = []
                    for dd in (d, d + 1):
                        w.append(wgu[along(1, dd)] if r == 0 else wx[r, lax.rem(y + dd, side)])
                    parts.append(jnp.concatenate(w, axis=1))
                acc = acc + dot(lhs[k // 2], jnp.concatenate(parts, axis=0))
            for i, dd in enumerate((d, d + 1)):
                piece = acc[:, i * LANES : (i + 1) * LANES]
                if dd == 0:
                    pkeep[span(g)] = piece
                else:
                    psrc[dd, span(g)] = piece.astype(BF16)
        for d in range(1, side):
            rcopy(psrc.at[d, span(g)], precv.at[side - d, span(g)], s_p, r_p.at[g], me, along(1, d)).start()
        got(q1r.at[g, pl.ds(1, side - 1)], r_q1.at[g])
        q1s[g] = q0[g] + q1r[g, 1] + q1r[g, 2] + q1r[g, 3]
        for d in range(1, side):
            rcopy(q1s.at[g], q2r.at[g, side - d], s_q2, r_q2.at[g], me, along(1, d)).start()

    lane = lax.broadcasted_iota(jnp.int32, (1, LANES), 1)

    def level7(g):
        per = SIZES[g]
        got(precv.at[pl.ds(1, side - 1), span(g)], r_p.at[g])
        total = pkeep[span(g)]
        for r in range(1, side):
            total = total + precv[r, span(g)].astype(F32)
        pback[pl.ds(START[g], per)] = total.astype(BF16).reshape(per, CAP, LANES)
        for i in range(per):
            s = START[g] + i
            if s == own:
                ret[me] = pback[s]
            else:
                rcopy(pback.at[s], ret.at[me], s_e, r_e, far(s), mt).start()
        got(q2r.at[g, pl.ds(1, side - 1)], r_q2.at[g])
        qtot = q1s[g] + q2r[g, 1] + q2r[g, 2] + q2r[g, 3]
        lines = [jnp.where(lane < CAP, pltpu.roll(qtot, (LANES - CAP * i) % LANES, 1), 0.0) for i in range(per)]
        lines = pltpu.roll(jnp.concatenate(lines, axis=0), lax.rem(me, LANES // CAP) * CAP, 1)
        for i in range(per):
            qsend[START[g] + i] = lines[i : i + 1]
        for i in range(per):
            s = START[g] + i
            if s == own:
                retq[me] = qsend[s]
            else:
                rcopy(qsend.at[s], retq.at[me], s_f, r_f, far(s), mt).start()

    def weight_grads(which):
        lhs = jnp.transpose((gsrc if which == 0 else hsrc)[...].astype(F32)).astype(BF16)
        for b in range(0, n_tp, 2):
            c = jnp.concatenate([rows[b + i, :, which].reshape(slots * CAP, LANES) for i in range(2)], axis=1)
            cols = slice(b * LANES, (b + 2) * LANES)
            if which == 0:
                r = dot(lhs, c)
                gg_out[0, :, cols] = r[:fh]
                ug_out[0, :, cols] = r[fh:]
            else:
                dg_out[0, :, cols] = dot(lhs[:fh], c)

    levels = [level0, level1, level2, level3, level4, level5, level6, level7]
    last = CHUNKS - 1
    for t in range(CHUNKS + 6):
        starts = [(0, g) for g in range(CHUNKS) if t == max(0, g - AHEAD)]
        for k, g in [(4, t - 4), (3, t - 3), (2, t - 2), (1, t - 1), *starts, (5, t - 4), (6, t - 5), (7, t - 6)]:
            if 0 <= g < CHUNKS:
                if (k, g) == (6, last):
                    with jax.named_scope("wg0"):
                        weight_grads(0)
                if (k, g) == (7, last):
                    with jax.named_scope("wg1"):
                        weight_grads(1)
                with jax.named_scope(f"L{k}g{g}"):
                    levels[k](g)

    with jax.named_scope("back"):
        got(ret.at[pl.ds(0, n_ep - 1)], r_e)
    tg_out[...] = dot(pickv[...], ret[...].reshape(n_ep * CAP, LANES)).astype(BF16)
    with jax.named_scope("backq"):
        got(retq.at[pl.ds(0, n_ep - 1)], r_f)
    group = LANES // CAP
    table = jnp.concatenate([jnp.sum(retq[a * group : (a + 1) * group], axis=0) for a in range(n_ep // group)], axis=1)
    table = jnp.broadcast_to(table, (8, n_ep * CAP))
    for k in range(2):
        r = dot(table, hot(k), precision=lax.Precision.HIGHEST)
        rg_out[k : k + 1, :] = r[:1] / wt[k]

    with jax.named_scope("drain"):
        got(send.at[pl.ds(0, n_ep - 1)], s_a)
        got(rows.at[pl.ds(0, n_tp - 1)], s_b)
        got(wx.at[pl.ds(1, side - 1)], s_w)
        got(grecv.at[pl.ds(1, side - 1)], s_g)
        got(precv.at[pl.ds(1, side - 1)], s_p)
        got(q1r.at[:, pl.ds(1, side - 1)], s_q1)
        got(q2r.at[:, pl.ds(1, side - 1)], s_q2)
        got(ret.at[pl.ds(0, n_ep - 1)], s_e)
        got(retq.at[pl.ds(0, n_ep - 1)], s_f)


def write_out(n, *refs):
    copies = [pltpu.make_async_copy(refs[i], refs[n + i], refs[2 * n].at[i]) for i in range(n)]
    for c in copies:
        c.start()
    for c in copies:
        c.wait()


def per_device(nz, tokens, cotangent, expert_ids, route_weight, gate_weight, up_weight, down_weight):
    side = SIDE
    n_ep, n_tp = 2 * nz, side * side
    all_rows = n_ep * CAP
    nt = tokens.shape[0]
    fh = gate_weight.shape[1]
    vmem = pl.BlockSpec(memory_space=pltpu.VMEM)
    hbm = pl.BlockSpec(memory_space=pltpu.HBM)
    dma = pltpu.SemaphoreType.DMA
    scratch = [
        pltpu.VMEM((2, nt), jnp.int32),
        pltpu.VMEM((2, nt), BF16),
        pltpu.VMEM((nt, LANES), BF16),
        pltpu.VMEM((nt, LANES), BF16),
        pltpu.VMEM((n_tp, LANES, LANES), BF16),
        pltpu.VMEM((n_tp, LANES, LANES), BF16),
        pltpu.VMEM((n_ep, 2, CAP, LANES), BF16),
        pltpu.VMEM((n_tp, n_ep, 2, CAP, LANES), BF16),
        pltpu.VMEM((side, side, LANES, LANES), BF16),
        pltpu.VMEM((all_rows, LANES), BF16),
        pltpu.VMEM((all_rows, LANES), BF16),
        pltpu.VMEM((side, all_rows, LANES), BF16),
        pltpu.VMEM((all_rows, LANES), F32),
        pltpu.VMEM((side, all_rows, LANES), BF16),
        pltpu.VMEM((side, all_rows, LANES), BF16),
        pltpu.VMEM((n_ep, CAP, LANES), BF16),
        pltpu.VMEM((CHUNKS, 1, LANES), F32),
        pltpu.VMEM((CHUNKS, side, 1, LANES), F32),
        pltpu.VMEM((CHUNKS, 1, LANES), F32),
        pltpu.VMEM((CHUNKS, side, 1, LANES), F32),
        pltpu.VMEM((n_ep, 1, LANES), F32),
        pltpu.VMEM((n_ep, CAP, LANES), BF16),
        pltpu.VMEM((n_ep, 1, LANES), F32),
        pltpu.VMEM((nt, n_ep * CAP), BF16),
        dma((2,)), dma((2,)), dma, dma,
        dma, dma((CHUNKS,)),
        dma, dma((2 * CHUNKS * n_tp,)),
        dma, dma,
        dma, dma((CHUNKS,)),
        dma, dma((CHUNKS,)),
        dma, dma((CHUNKS,)),
        dma, dma((CHUNKS,)),
        dma, dma,
        dma, dma,
    ]
    shapes = [((nt, LANES), BF16), ((2, nt), F32)] + [(gate_weight.shape, F32)] * 3
    ins = (tokens, cotangent, expert_ids.T, route_weight.T, gate_weight, up_weight, down_weight)
    made = pl.pallas_call(
        functools.partial(kernel, nz),
        out_shape=tuple(pltpu.VMEM(*a) for a in shapes),
        in_specs=[hbm] * 7,
        out_specs=(vmem,) * 5,
        scratch_shapes=scratch,
        compiler_params=pltpu.CompilerParams(collective_id=0, has_side_effects=True, vmem_limit_bytes=24 * 1024 * 1024),
    )(*(pltpu.with_memory_space_constraint(a, pltpu.HBM) for a in ins))
    tg, rg, *grads = pl.pallas_call(
        functools.partial(write_out, 5),
        out_shape=tuple(pltpu.HBM(*a) for a in shapes),
        in_specs=[vmem] * 5,
        out_specs=(hbm,) * 5,
        scratch_shapes=[dma((5,))],
        compiler_params=pltpu.CompilerParams(vmem_limit_bytes=1024 * 1024),
    )(*(pltpu.with_memory_space_constraint(a, pltpu.VMEM) for a in made))
    return (tg, rg.T, *grads)


def solution(mesh):
    nz = mesh.shape["ep"] // 2
    in_specs = (
        P("ep", None), P("ep", None), P("ep", None), P("ep", None),
        P("ep", "tp", None), P("ep", "tp", None), P("ep", "tp", None),
    )
    out_specs = (
        P("ep", "tp"), P("ep", None), P("ep", "tp", None), P("ep", "tp", None), P("ep", "tp", None),
    )
    return jax.shard_map(
        functools.partial(per_device, nz), mesh=mesh, in_specs=in_specs, out_specs=out_specs, check_vma=False
    )
```

```python
import functools

import jax
import jax.numpy as jnp
from jax import lax
from jax.experimental import pallas as pl
from jax.experimental.pallas import tpu as pltpu
from jax.sharding import PartitionSpec as P

MESH = pl.DeviceIdType.MESH
F32, BF16 = jnp.float32, jnp.bfloat16
CAP = 16
LANES = 128
SIZES = (8, 8, 8, 8)
CHUNKS = len(SIZES)
START = tuple(sum(SIZES[:g]) for g in range(CHUNKS))
SIDE = 4


def dot(a, b, dims=((1,), (0,)), **kw):
    return lax.dot_general(a, b, (dims, ((), ())), preferred_element_type=F32, **kw)


def slot_order(nz):
    near = [0] + [d for k in range(1, nz // 2) for d in (k, nz - k)] + [nz // 2]
    n = nz // 4
    return near[:n] + near[2 * n : 3 * n] + near[n : 2 * n] + near[3 * n :]


FIRST_AXIS = (0, 1) * CHUNKS
FIRST_STEP = (1, 1, -1, -1) * CHUNKS
DIRECT1 = tuple(range(2 * CHUNKS))
XPART = (4, 4, 4, 4)
DIRECT2 = ()
WPARTS, WFIRST = 1, 1
PROGRAM = (
    (0, 0), (1, 0), (0, 1), (2, 0), (1, 1), (0, 3), (3, 0), (2, 1), (1, 3), (0, 2), (5, 0), (3, 1), (2, 3), (1, 2), (5, 1),
    (6, 0), (3, 3), (5, 3), (2, 2), (6, 1), (7, 0), (6, 3), (3, 2), (5, 2), (7, 1), (8, 0), (7, 3), (6, 2), (8, 1), (7, 2),
)


def kernel(nz, tok, cot, ids_hbm, rw_hbm, gw, uw, dw, tg_out, rg_out, gg_out, ug_out, dg_out,
           ids_ref, rw_ref, tokc, cotc, wgu, wd, send, rows, wx, gsrc, hsrc, grecv, pkeep, psrc, precv,
           pback, q0, q1r, q1s, q2r, qsend, ret, retq, pickv,
           sem_i, sem_tc, sem_w, sem_wd, s_a, r_a, s_b, r_b, s_w, r_w, s_g, r_g, s_p, r_p,
           s_q1, r_q1, s_q2, r_q2, s_e, r_e, s_f, r_f):
    side = SIDE
    n_ep, n_tp = 2 * nz, side * side
    order = slot_order(nz)
    slots = n_ep
    own = 2 * order.index(0)
    assert own in START and sum(SIZES) == slots
    me, mt = lax.axis_index("ep"), lax.axis_index("tp")
    z, core = me // 2, lax.rem(me, 2)
    y, x = mt // side, lax.rem(mt, side)
    fh = gw.shape[1]
    nt = tokc.shape[0]

    col = pl.ds(pl.multiple_of(mt * LANES, LANES), LANES)
    load_i = pltpu.make_async_copy(ids_hbm, ids_ref, sem_i.at[0])
    load_r = pltpu.make_async_copy(rw_hbm, rw_ref, sem_i.at[1])
    load_t = pltpu.make_async_copy(tok.at[:, col], tokc, sem_tc.at[0])
    load_c = pltpu.make_async_copy(cot.at[:, col], cotc, sem_tc.at[1])
    for load in (load_i, load_r, load_t, load_c):
        load.start()

    def at(dx, dy):
        return lax.rem(y + dy, side) * side + lax.rem(x + dx, side)

    def along(axis, d):
        return at(d, 0) if axis == 0 else at(0, d)

    def far(slot):
        return lax.rem(z + order[slot // 2], nz) * 2 + lax.rem(core + slot % 2, 2)

    def back_slot(slot):
        return 2 * order.index((nz - order[slot // 2]) % nz) + slot % 2

    def rcopy(src, dst, ssem, rsem, ep, tp):
        return pltpu.make_async_remote_copy(
            src_ref=src, dst_ref=dst, send_sem=ssem, recv_sem=rsem,
            device_id={"ep": ep, "tp": tp}, device_id_type=MESH,
        )

    def got(ref, rsem):
        pltpu.make_async_copy(ref, ref, rsem).wait()

    barrier = pltpu.get_barrier_semaphore()

    def greet(i, carry):
        pl.semaphore_signal(barrier, inc=1, device_id={"ep": lax.rem(me + i, n_ep), "tp": mt}, device_id_type=MESH)
        return carry

    lax.fori_loop(1, n_ep, greet, 0)
    for d in range(1, side):
        for axis in range(2):
            pl.semaphore_signal(barrier, inc=1, device_id={"ep": me, "tp": along(axis, d)}, device_id_type=MESH)

    for b in range(n_tp):
        cols = pl.ds(b * LANES, LANES)
        pltpu.make_async_copy(gw.at[0, :, cols], wgu.at[b, pl.ds(0, fh)], sem_w).start()
        pltpu.make_async_copy(uw.at[0, :, cols], wgu.at[b, pl.ds(fh, fh)], sem_w).start()

    load_i.wait()
    load_r.wait()
    ids = [ids_ref[k : k + 1, :] for k in range(2)]
    wt = [rw_ref[k : k + 1, :].astype(F32) for k in range(2)]
    e_row = lax.broadcasted_iota(jnp.int32, (n_ep, nt), 0)
    mem = [(e_row == ids[k]).astype(F32) for k in range(2)]
    upper = (lax.broadcasted_iota(jnp.int32, (nt, nt), 0) < lax.broadcasted_iota(jnp.int32, (nt, nt), 1)).astype(BF16)
    before = dot((mem[0] + mem[1]).astype(BF16), upper)
    rank = [jnp.sum(mem[k] * before, axis=0, keepdims=True).astype(jnp.int32) for k in range(2)]
    place_of = [ids[k] * CAP + rank[k] for k in range(2)]

    def hot(k):
        return (lax.broadcasted_iota(jnp.int32, (n_ep * CAP, nt), 0) == place_of[k]).astype(F32)

    h0, h1 = hot(0), hot(1)
    pick_t = h0 + h1
    scaled_t = h0 * wt[0] + h1 * wt[1]
    load_t.wait()
    load_c.wait()
    send[:, 0] = dot(pick_t.astype(BF16), tokc[...]).astype(BF16).reshape(n_ep, CAP, LANES)
    send[:, 1] = dot(scaled_t.astype(BF16), cotc[...]).astype(BF16).reshape(n_ep, CAP, LANES)
    rows[mt, own] = send[me]
    got(wgu, sem_w)

    with jax.named_scope("bar"):
        pl.semaphore_wait(barrier, n_ep - 1 + 2 * (side - 1))

    def dispatch(chunk):
        for s in range(START[chunk], START[chunk] + SIZES[chunk]):
            if s != own:
                e = far(back_slot(s))
                rcopy(send.at[e], rows.at[mt, s], s_a, r_a.at[chunk], e, mt).start()

    dispatch(0)

    def weights_out(part):
        w4 = wgu.reshape(side, side, LANES, LANES)
        some = pl.ds(part * side // WPARTS, side // WPARTS)
        for d in range(1, side):
            rcopy(w4.at[some, lax.rem(x + d, side)], wx.at[side - d, some], s_w, r_w, me, along(0, d)).start()

    for part in range(WFIRST):
        weights_out(part)
    for b in range(n_tp):
        cols = pl.ds(b * LANES, LANES)
        for h in range(2):
            pltpu.make_async_copy(dw.at[0, :, cols], wd.at[b, pl.ds(h * fh, fh)], sem_wd).start()
    pickv[...] = jnp.transpose(pick_t).astype(BF16)
    got(wd, sem_wd)
    for chunk in (1, 3, 2):
        dispatch(chunk)

    def ref_of(q, du, dv):
        b = at(du, dv) if FIRST_AXIS[q] == 0 else at(dv, du)
        g = q // 2
        n = XPART[g]
        return rows.at[b, pl.ds(START[g] + n, SIZES[g] - n) if q % 2 else pl.ds(START[g], n)]

    def span(g):
        return pl.ds(START[g] * CAP, SIZES[g] * CAP)

    def pass_on(q, du, dv, second, step):
        rdu, rdv = (du, (dv - step) % side) if second else ((du - step) % side, dv)
        axis = FIRST_AXIS[q] ^ int(second)
        ref = ref_of(q, du, dv)
        rcopy(ref, ref, s_b, r_b.at[(q * side + rdu) * side + rdv], me, along(axis, step % side)).start()

    def block(q, du, dv):
        got(ref_of(q, du, dv), r_b.at[(q * side + du) * side + dv])

    def both(q, du, dv, second):
        pass_on(q, du, dv, second, 1)
        pass_on(q, du, dv, second, -1)

    def relay(q, keep, second):
        step = FIRST_STEP[q] if not second else 1 if (q + keep) % 2 == 0 else -1
        v = side - 1 if step == 1 else 1
        pass_on(q, *((keep, v) if second else (v, keep)), second, step)

    def spread(q, du):
        both(q, du, 0, True)
        if q in DIRECT2:
            pass_on(q, du, 0, True, 2)

    def halves(g):
        return (2 * g, 2 * g + 1)

    def level0(g):
        skip = 1 if START[g] == own else 0
        got(rows.at[mt, pl.ds(START[g] + skip, SIZES[g] - skip)], r_a.at[g])
        for q in halves(g):
            both(q, 0, 0, False)
            if q in DIRECT1:
                pass_on(q, 0, 0, False, 2)
        for q in halves(g):
            spread(q, 0)

    def second_in(q, du):
        if q not in DIRECT2:
            block(q, du, 1)
            block(q, du, side - 1)
            relay(q, du, True)

    def level1(g):
        for q in halves(g):
            for du in (1, side - 1):
                block(q, du, 0)
                spread(q, du)
            if q not in DIRECT1:
                relay(q, 0, False)
        for q in halves(g):
            block(q, 2, 0)
            spread(q, 2)

    def level2(g):
        for du in (0, 1, side - 1, 2):
            for q in halves(g):
                second_in(q, du)

    def level3(g):
        for q in halves(g):
            for du in range(side):
                if q in DIRECT2:
                    block(q, du, 1)
                    block(q, du, side - 1)
                block(q, du, 2)

    def level5(g):
        per = SIZES[g]
        crows = per * CAP
        half = lax.broadcasted_iota(jnp.int32, (crows, LANES), 1) < fh
        pre = jnp.zeros((crows, LANES), F32)
        back = jnp.zeros((crows, LANES), F32)
        for b in range(0, n_tp, 2):
            a = [rows[b + i, pl.ds(START[g], per)] for i in range(2)]
            t = jnp.concatenate([a[i][:, 0].reshape(crows, LANES) for i in range(2)], axis=1)
            c = jnp.concatenate([a[i][:, 1].reshape(crows, LANES) for i in range(2)], axis=1)
            wt_b = jnp.concatenate([wgu[b], wgu[b + 1]], axis=1)
            wd_b = jnp.concatenate([wd[b], wd[b + 1]], axis=1)
            pre = pre + dot(t, wt_b, ((1,), (1,)))
            back = back + dot(c, wd_b, ((1,), (1,)))
        other = pltpu.roll(pre, fh, 1)
        gate = jnp.where(half, pre, other)
        up = jnp.where(half, other, pre)
        sig = jax.nn.sigmoid(gate)
        silu = gate * sig
        hidden = silu * up
        grad = back * jnp.where(half, up * sig * (1.0 + gate * (1.0 - sig)), silu)
        gsrc[span(g)] = grad.astype(BF16)
        hsrc[span(g)] = hidden.astype(BF16)
        prod = jnp.where(half, hidden * back, 0.0)
        if crows < LANES:
            prod = jnp.concatenate([prod, jnp.zeros((LANES - crows, LANES), F32)], axis=0)
        prod = jnp.transpose(prod)
        q0[g] = jnp.sum(prod, axis=0, keepdims=True)
        for d in range(1, side):
            rcopy(gsrc.at[span(g)], grecv.at[side - d, span(g)], s_g, r_g.at[g], me, along(0, d)).start()
        for d in range(1, side):
            rcopy(q0.at[g], q1r.at[g, side - d], s_q1, r_q1.at[g], me, along(0, d)).start()

    def level6(g):
        if g == 0:
            got(wx.at[pl.ds(1, side - 1)], r_w)
        crows = SIZES[g] * CAP
        got(q1r.at[g, pl.ds(1, side - 1)], r_q1.at[g])
        q1s[g] = q0[g] + q1r[g, 1] + q1r[g, 2] + q1r[g, 3]
        for d in range(1, side):
            rcopy(q1s.at[g], q2r.at[g, side - d], s_q2, r_q2.at[g], me, along(1, d)).start()
        got(grecv.at[pl.ds(1, side - 1), span(g)], r_g.at[g])
        lhs = [gsrc[span(g)]] + [grecv[r, span(g)] for r in range(1, side)]
        lhs = [jnp.concatenate(lhs[k : k + 2], axis=1) for k in range(0, side, 2)]
        for d in reversed(range(0, side, 2)):
            acc = jnp.zeros((crows, 2 * LANES), F32)
            for k in range(0, side, 2):
                parts = []
                for r in (k, k + 1):
                    w = []
                    for dd in (d, d + 1):
                        w.append(wgu[along(1, dd)] if r == 0 else wx[r, lax.rem(y + dd, side)])
                    parts.append(jnp.concatenate(w, axis=1))
                acc = acc + dot(lhs[k // 2], jnp.concatenate(parts, axis=0))
            for i, dd in enumerate((d, d + 1)):
                piece = acc[:, i * LANES : (i + 1) * LANES]
                if dd == 0:
                    pkeep[span(g)] = piece
                else:
                    psrc[dd, span(g)] = piece.astype(BF16)
        for d in range(1, side):
            rcopy(psrc.at[d, span(g)], precv.at[side - d, span(g)], s_p, r_p.at[g], me, along(1, d)).start()

    lane = lax.broadcasted_iota(jnp.int32, (1, LANES), 1)

    def level7(g):
        per = SIZES[g]
        got(q2r.at[g, pl.ds(1, side - 1)], r_q2.at[g])
        qtot = q1s[g] + q2r[g, 1] + q2r[g, 2] + q2r[g, 3]
        lines = [jnp.where(lane < CAP, pltpu.roll(qtot, (LANES - CAP * i) % LANES, 1), 0.0) for i in range(per)]
        lines = pltpu.roll(jnp.concatenate(lines, axis=0), lax.rem(me, LANES // CAP) * CAP, 1)
        for i in range(per):
            qsend[START[g] + i] = lines[i : i + 1]
        for i in range(per):
            s = START[g] + i
            if s == own:
                retq[me] = qsend[s]
            else:
                rcopy(qsend.at[s], retq.at[me], s_f, r_f, far(s), mt).start()
        got(precv.at[pl.ds(1, side - 1), span(g)], r_p.at[g])
        total = pkeep[span(g)]
        for r in range(1, side):
            total = total + precv[r, span(g)].astype(F32)
        pback[pl.ds(START[g], per)] = total.astype(BF16).reshape(per, CAP, LANES)
        for i in range(per):
            s = START[g] + i
            if s == own:
                ret[me] = pback[s]
            else:
                rcopy(pback.at[s], ret.at[me], s_e, r_e, far(s), mt).start()

    def weight_grads(which):
        lhs = jnp.transpose((gsrc if which == 0 else hsrc)[...].astype(F32)).astype(BF16)
        for b in range(0, n_tp, 2):
            c = jnp.concatenate([rows[b + i, :, which].reshape(slots * CAP, LANES) for i in range(2)], axis=1)
            cols = slice(b * LANES, (b + 2) * LANES)
            if which == 0:
                r = dot(lhs, c)
                gg_out[0, :, cols] = r[:fh]
                ug_out[0, :, cols] = r[fh:]
            else:
                dg_out[0, :, cols] = dot(lhs[:fh], c)

    levels = {0: level0, 1: level1, 2: level2, 3: level3, 5: level5, 6: level6, 7: level7, 8: weight_grads, 9: weights_out}
    for k, g in PROGRAM:
        with jax.named_scope(f"L{k}g{g}"):
            levels[k](g)

    with jax.named_scope("backq"):
        got(retq.at[pl.ds(0, n_ep - 1)], r_f)
    group = LANES // CAP
    table = jnp.concatenate([jnp.sum(retq[a * group : (a + 1) * group], axis=0) for a in range(n_ep // group)], axis=1)
    table = jnp.broadcast_to(table, (8, n_ep * CAP))
    for k in range(2):
        r = dot(table, hot(k), precision=lax.Precision.HIGHEST)
        rg_out[k : k + 1, :] = r[:1] / wt[k]

    with jax.named_scope("back"):
        got(ret.at[pl.ds(0, n_ep - 1)], r_e)
    tg_out[...] = dot(pickv[...], ret[...].reshape(n_ep * CAP, LANES)).astype(BF16)

    with jax.named_scope("drain"):
        got(send.at[pl.ds(0, n_ep - 1)], s_a)
        got(rows.at[pl.ds(0, n_tp - 1)], s_b)
        got(wx.at[pl.ds(1, side - 1)], s_w)
        got(grecv.at[pl.ds(1, side - 1)], s_g)
        got(precv.at[pl.ds(1, side - 1)], s_p)
        got(q1r.at[:, pl.ds(1, side - 1)], s_q1)
        got(q2r.at[:, pl.ds(1, side - 1)], s_q2)
        got(ret.at[pl.ds(0, n_ep - 1)], s_e)
        got(retq.at[pl.ds(0, n_ep - 1)], s_f)


def write_out(n, *refs):
    copies = [pltpu.make_async_copy(refs[i], refs[n + i], refs[2 * n].at[i]) for i in range(n)]
    for c in copies:
        c.start()
    for c in copies:
        c.wait()


def per_device(nz, tokens, cotangent, expert_ids, route_weight, gate_weight, up_weight, down_weight):
    side = SIDE
    n_ep, n_tp = 2 * nz, side * side
    all_rows = n_ep * CAP
    nt = tokens.shape[0]
    fh = gate_weight.shape[1]
    vmem = pl.BlockSpec(memory_space=pltpu.VMEM)
    hbm = pl.BlockSpec(memory_space=pltpu.HBM)
    dma = pltpu.SemaphoreType.DMA
    scratch = [
        pltpu.VMEM((2, nt), jnp.int32),
        pltpu.VMEM((2, nt), BF16),
        pltpu.VMEM((nt, LANES), BF16),
        pltpu.VMEM((nt, LANES), BF16),
        pltpu.VMEM((n_tp, LANES, LANES), BF16),
        pltpu.VMEM((n_tp, LANES, LANES), BF16),
        pltpu.VMEM((n_ep, 2, CAP, LANES), BF16),
        pltpu.VMEM((n_tp, n_ep, 2, CAP, LANES), BF16),
        pltpu.VMEM((side, side, LANES, LANES), BF16),
        pltpu.VMEM((all_rows, LANES), BF16),
        pltpu.VMEM((all_rows, LANES), BF16),
        pltpu.VMEM((side, all_rows, LANES), BF16),
        pltpu.VMEM((all_rows, LANES), F32),
        pltpu.VMEM((side, all_rows, LANES), BF16),
        pltpu.VMEM((side, all_rows, LANES), BF16),
        pltpu.VMEM((n_ep, CAP, LANES), BF16),
        pltpu.VMEM((CHUNKS, 1, LANES), F32),
        pltpu.VMEM((CHUNKS, side, 1, LANES), F32),
        pltpu.VMEM((CHUNKS, 1, LANES), F32),
        pltpu.VMEM((CHUNKS, side, 1, LANES), F32),
        pltpu.VMEM((n_ep, 1, LANES), F32),
        pltpu.VMEM((n_ep, CAP, LANES), BF16),
        pltpu.VMEM((n_ep, 1, LANES), F32),
        pltpu.VMEM((nt, n_ep * CAP), BF16),
        dma((2,)), dma((2,)), dma, dma,
        dma, dma((CHUNKS,)),
        dma, dma((2 * CHUNKS * n_tp,)),
        dma, dma,
        dma, dma((CHUNKS,)),
        dma, dma((CHUNKS,)),
        dma, dma((CHUNKS,)),
        dma, dma((CHUNKS,)),
        dma, dma,
        dma, dma,
    ]
    shapes = [((nt, LANES), BF16), ((2, nt), F32)] + [(gate_weight.shape, F32)] * 3
    ins = (tokens, cotangent, expert_ids.T, route_weight.T, gate_weight, up_weight, down_weight)
    made = pl.pallas_call(
        functools.partial(kernel, nz),
        out_shape=tuple(pltpu.VMEM(*a) for a in shapes),
        in_specs=[hbm] * 7,
        out_specs=(vmem,) * 5,
        scratch_shapes=scratch,
        compiler_params=pltpu.CompilerParams(collective_id=0, has_side_effects=True, vmem_limit_bytes=24 * 1024 * 1024),
    )(*(pltpu.with_memory_space_constraint(a, pltpu.HBM) for a in ins))
    tg, rg, *grads = pl.pallas_call(
        functools.partial(write_out, 5),
        out_shape=tuple(pltpu.HBM(*a) for a in shapes),
        in_specs=[vmem] * 5,
        out_specs=(hbm,) * 5,
        scratch_shapes=[dma((5,))],
        compiler_params=pltpu.CompilerParams(vmem_limit_bytes=1024 * 1024),
    )(*(pltpu.with_memory_space_constraint(a, pltpu.VMEM) for a in made))
    return (tg, rg.T, *grads)


def solution(mesh):
    nz = mesh.shape["ep"] // 2
    in_specs = (
        P("ep", None), P("ep", None), P("ep", None), P("ep", None),
        P("ep", "tp", None), P("ep", "tp", None), P("ep", "tp", None),
    )
    out_specs = (
        P("ep", "tp"), P("ep", None), P("ep", "tp", None), P("ep", "tp", None), P("ep", "tp", None),
    )
    return jax.shard_map(
        functools.partial(per_device, nz), mesh=mesh, in_specs=in_specs, out_specs=out_specs, check_vma=False
    )
```

```python
import functools

import jax
import jax.numpy as jnp
from jax import lax
from jax.experimental import pallas as pl
from jax.experimental.pallas import tpu as pltpu
from jax.sharding import PartitionSpec as P

MESH = pl.DeviceIdType.MESH
F32, BF16 = jnp.float32, jnp.bfloat16
CAP = 16
LANES = 128
SIZES = (8, 8, 8, 8)
CHUNKS = len(SIZES)
START = tuple(sum(SIZES[:g]) for g in range(CHUNKS))
SIDE = 4


def dot(a, b, dims=((1,), (0,)), **kw):
    return lax.dot_general(a, b, (dims, ((), ())), preferred_element_type=F32, **kw)


def slot_order(nz):
    near = [0] + [d for k in range(1, nz // 2) for d in (k, nz - k)] + [nz // 2]
    n = nz // 4
    return near[:n] + near[2 * n : 3 * n] + near[n : 2 * n] + near[3 * n :]


FIRST_AXIS = (0, 1) * CHUNKS
FIRST_STEP = (1, 1, -1, -1) * CHUNKS
DIRECT1 = tuple(range(2 * CHUNKS))
XPART = (4, 5, 5, 5)
DIRECT2 = ()
WPARTS, WFIRST = 1, 1
PROGRAM = (
    (0, 0), (1, 0), (0, 1), (2, 0), (1, 1), (0, 3), (3, 0), (2, 1), (1, 3), (0, 2), (5, 0), (3, 1), (2, 3), (1, 2), (5, 1),
    (6, 0), (3, 3), (5, 3), (2, 2), (6, 1), (7, 0), (6, 3), (3, 2), (5, 2), (7, 1), (8, 0), (7, 3), (6, 2), (8, 1), (7, 2),
)


def kernel(nz, tok, cot, ids_hbm, rw_hbm, gw, uw, dw, tg_out, rg_out, gg_out, ug_out, dg_out,
           ids_ref, rw_ref, tokc, cotc, wgu, wd, send, rows, wx, gsrc, hsrc, grecv, pkeep, psrc, precv,
           pback, q0, q1r, q1s, q2r, qsend, ret, retq, pickv,
           sem_i, sem_tc, sem_w, sem_wd, s_a, r_a, s_b, r_b, s_w, r_w, s_g, r_g, s_p, r_p,
           s_q1, r_q1, s_q2, r_q2, s_e, r_e, s_f, r_f):
    side = SIDE
    n_ep, n_tp = 2 * nz, side * side
    order = slot_order(nz)
    slots = n_ep
    own = 2 * order.index(0)
    assert own in START and sum(SIZES) == slots
    me, mt = lax.axis_index("ep"), lax.axis_index("tp")
    z, core = me // 2, lax.rem(me, 2)
    y, x = mt // side, lax.rem(mt, side)
    fh = gw.shape[1]
    nt = tokc.shape[0]

    col = pl.ds(pl.multiple_of(mt * LANES, LANES), LANES)
    load_i = pltpu.make_async_copy(ids_hbm, ids_ref, sem_i.at[0])
    load_r = pltpu.make_async_copy(rw_hbm, rw_ref, sem_i.at[1])
    load_t = pltpu.make_async_copy(tok.at[:, col], tokc, sem_tc.at[0])
    load_c = pltpu.make_async_copy(cot.at[:, col], cotc, sem_tc.at[1])
    for load in (load_i, load_r, load_t, load_c):
        load.start()

    def at(dx, dy):
        return lax.rem(y + dy, side) * side + lax.rem(x + dx, side)

    def along(axis, d):
        return at(d, 0) if axis == 0 else at(0, d)

    def far(slot):
        return lax.rem(z + order[slot // 2], nz) * 2 + lax.rem(core + slot % 2, 2)

    def back_slot(slot):
        return 2 * order.index((nz - order[slot // 2]) % nz) + slot % 2

    def rcopy(src, dst, ssem, rsem, ep, tp):
        return pltpu.make_async_remote_copy(
            src_ref=src, dst_ref=dst, send_sem=ssem, recv_sem=rsem,
            device_id={"ep": ep, "tp": tp}, device_id_type=MESH,
        )

    def got(ref, rsem):
        pltpu.make_async_copy(ref, ref, rsem).wait()

    barrier = pltpu.get_barrier_semaphore()

    def greet(i, carry):
        pl.semaphore_signal(barrier, inc=1, device_id={"ep": lax.rem(me + i, n_ep), "tp": mt}, device_id_type=MESH)
        return carry

    lax.fori_loop(1, n_ep, greet, 0)
    for d in range(1, side):
        for axis in range(2):
            pl.semaphore_signal(barrier, inc=1, device_id={"ep": me, "tp": along(axis, d)}, device_id_type=MESH)

    for b in range(n_tp):
        cols = pl.ds(b * LANES, LANES)
        pltpu.make_async_copy(gw.at[0, :, cols], wgu.at[b, pl.ds(0, fh)], sem_w).start()
        pltpu.make_async_copy(uw.at[0, :, cols], wgu.at[b, pl.ds(fh, fh)], sem_w).start()

    load_i.wait()
    load_r.wait()
    ids = [ids_ref[k : k + 1, :] for k in range(2)]
    wt = [rw_ref[k : k + 1, :].astype(F32) for k in range(2)]
    e_row = lax.broadcasted_iota(jnp.int32, (n_ep, nt), 0)
    mem = [(e_row == ids[k]).astype(F32) for k in range(2)]
    upper = (lax.broadcasted_iota(jnp.int32, (nt, nt), 0) < lax.broadcasted_iota(jnp.int32, (nt, nt), 1)).astype(BF16)
    before = dot((mem[0] + mem[1]).astype(BF16), upper)
    rank = [jnp.sum(mem[k] * before, axis=0, keepdims=True).astype(jnp.int32) for k in range(2)]
    place_of = [ids[k] * CAP + rank[k] for k in range(2)]

    def hot(k):
        return (lax.broadcasted_iota(jnp.int32, (n_ep * CAP, nt), 0) == place_of[k]).astype(F32)

    h0, h1 = hot(0), hot(1)
    pick_t = h0 + h1
    scaled_t = h0 * wt[0] + h1 * wt[1]
    load_t.wait()
    load_c.wait()
    send[:, 0] = dot(pick_t.astype(BF16), tokc[...]).astype(BF16).reshape(n_ep, CAP, LANES)
    send[:, 1] = dot(scaled_t.astype(BF16), cotc[...]).astype(BF16).reshape(n_ep, CAP, LANES)
    rows[mt, own] = send[me]
    got(wgu, sem_w)

    with jax.named_scope("bar"):
        pl.semaphore_wait(barrier, n_ep - 1 + 2 * (side - 1))

    def dispatch(chunk):
        for s in range(START[chunk], START[chunk] + SIZES[chunk]):
            if s != own:
                e = far(back_slot(s))
                rcopy(send.at[e], rows.at[mt, s], s_a, r_a.at[chunk], e, mt).start()

    dispatch(0)

    def weights_out(part):
        w4 = wgu.reshape(side, side, LANES, LANES)
        some = pl.ds(part * side // WPARTS, side // WPARTS)
        for d in range(1, side):
            rcopy(w4.at[some, lax.rem(x + d, side)], wx.at[side - d, some], s_w, r_w, me, along(0, d)).start()

    for part in range(WFIRST):
        weights_out(part)
    for b in range(n_tp):
        cols = pl.ds(b * LANES, LANES)
        for h in range(2):
            pltpu.make_async_copy(dw.at[0, :, cols], wd.at[b, pl.ds(h * fh, fh)], sem_wd).start()
    pickv[...] = jnp.transpose(pick_t).astype(BF16)
    got(wd, sem_wd)
    for chunk in (1, 3, 2):
        dispatch(chunk)

    def ref_of(q, du, dv):
        b = at(du, dv) if FIRST_AXIS[q] == 0 else at(dv, du)
        g = q // 2
        n = XPART[g]
        return rows.at[b, pl.ds(START[g] + n, SIZES[g] - n) if q % 2 else pl.ds(START[g], n)]

    def span(g):
        return pl.ds(START[g] * CAP, SIZES[g] * CAP)

    def pass_on(q, du, dv, second, step):
        rdu, rdv = (du, (dv - step) % side) if second else ((du - step) % side, dv)
        axis = FIRST_AXIS[q] ^ int(second)
        ref = ref_of(q, du, dv)
        rcopy(ref, ref, s_b, r_b.at[(q * side + rdu) * side + rdv], me, along(axis, step % side)).start()

    def block(q, du, dv):
        got(ref_of(q, du, dv), r_b.at[(q * side + du) * side + dv])

    def both(q, du, dv, second):
        pass_on(q, du, dv, second, 1)
        pass_on(q, du, dv, second, -1)

    def relay(q, keep, second):
        step = FIRST_STEP[q] if not second else 1 if (q + keep) % 2 == 0 else -1
        v = side - 1 if step == 1 else 1
        pass_on(q, *((keep, v) if second else (v, keep)), second, step)

    def spread(q, du):
        both(q, du, 0, True)
        if q in DIRECT2:
            pass_on(q, du, 0, True, 2)

    def halves(g):
        return (2 * g, 2 * g + 1)

    def level0(g):
        skip = 1 if START[g] == own else 0
        got(rows.at[mt, pl.ds(START[g] + skip, SIZES[g] - skip)], r_a.at[g])
        for q in halves(g):
            both(q, 0, 0, False)
            if q in DIRECT1:
                pass_on(q, 0, 0, False, 2)
        for q in halves(g):
            spread(q, 0)

    def second_in(q, du):
        if q not in DIRECT2:
            block(q, du, 1)
            block(q, du, side - 1)
            relay(q, du, True)

    def level1(g):
        for q in halves(g):
            for du in (1, side - 1):
                block(q, du, 0)
                spread(q, du)
            if q not in DIRECT1:
                relay(q, 0, False)
        for q in halves(g):
            block(q, 2, 0)
            spread(q, 2)

    def level2(g):
        for du in (0, 1, side - 1, 2):
            for q in halves(g):
                second_in(q, du)

    def level3(g):
        for q in halves(g):
            for du in range(side):
                if q in DIRECT2:
                    block(q, du, 1)
                    block(q, du, side - 1)
                block(q, du, 2)

    def level5(g):
        per = SIZES[g]
        crows = per * CAP
        half = lax.broadcasted_iota(jnp.int32, (crows, LANES), 1) < fh
        pre = jnp.zeros((crows, LANES), F32)
        back = jnp.zeros((crows, LANES), F32)
        for b in range(0, n_tp, 2):
            a = [rows[b + i, pl.ds(START[g], per)] for i in range(2)]
            t = jnp.concatenate([a[i][:, 0].reshape(crows, LANES) for i in range(2)], axis=1)
            c = jnp.concatenate([a[i][:, 1].reshape(crows, LANES) for i in range(2)], axis=1)
            wt_b = jnp.concatenate([wgu[b], wgu[b + 1]], axis=1)
            wd_b = jnp.concatenate([wd[b], wd[b + 1]], axis=1)
            pre = pre + dot(t, wt_b, ((1,), (1,)))
            back = back + dot(c, wd_b, ((1,), (1,)))
        other = pltpu.roll(pre, fh, 1)
        gate = jnp.where(half, pre, other)
        up = jnp.where(half, other, pre)
        sig = jax.nn.sigmoid(gate)
        silu = gate * sig
        hidden = silu * up
        grad = back * jnp.where(half, up * sig * (1.0 + gate * (1.0 - sig)), silu)
        gsrc[span(g)] = grad.astype(BF16)
        hsrc[span(g)] = hidden.astype(BF16)
        prod = jnp.where(half, hidden * back, 0.0)
        if crows < LANES:
            prod = jnp.concatenate([prod, jnp.zeros((LANES - crows, LANES), F32)], axis=0)
        prod = jnp.transpose(prod)
        q0[g] = jnp.sum(prod, axis=0, keepdims=True)
        for d in range(1, side):
            rcopy(gsrc.at[span(g)], grecv.at[side - d, span(g)], s_g, r_g.at[g], me, along(0, d)).start()
        for d in range(1, side):
            rcopy(q0.at[g], q1r.at[g, side - d], s_q1, r_q1.at[g], me, along(0, d)).start()

    def level6(g):
        if g == 0:
            got(wx.at[pl.ds(1, side - 1)], r_w)
        crows = SIZES[g] * CAP
        got(q1r.at[g, pl.ds(1, side - 1)], r_q1.at[g])
        q1s[g] = q0[g] + q1r[g, 1] + q1r[g, 2] + q1r[g, 3]
        for d in range(1, side):
            rcopy(q1s.at[g], q2r.at[g, side - d], s_q2, r_q2.at[g], me, along(1, d)).start()
        got(grecv.at[pl.ds(1, side - 1), span(g)], r_g.at[g])
        lhs = [gsrc[span(g)]] + [grecv[r, span(g)] for r in range(1, side)]
        lhs = [jnp.concatenate(lhs[k : k + 2], axis=1) for k in range(0, side, 2)]
        for d in reversed(range(0, side, 2)):
            acc = jnp.zeros((crows, 2 * LANES), F32)
            for k in range(0, side, 2):
                parts = []
                for r in (k, k + 1):
                    w = []
                    for dd in (d, d + 1):
                        w.append(wgu[along(1, dd)] if r == 0 else wx[r, lax.rem(y + dd, side)])
                    parts.append(jnp.concatenate(w, axis=1))
                acc = acc + dot(lhs[k // 2], jnp.concatenate(parts, axis=0))
            for i, dd in enumerate((d, d + 1)):
                piece = acc[:, i * LANES : (i + 1) * LANES]
                if dd == 0:
                    pkeep[span(g)] = piece
                else:
                    psrc[dd, span(g)] = piece.astype(BF16)
        for d in range(1, side):
            rcopy(psrc.at[d, span(g)], precv.at[side - d, span(g)], s_p, r_p.at[g], me, along(1, d)).start()

    lane = lax.broadcasted_iota(jnp.int32, (1, LANES), 1)

    def level7(g):
        per = SIZES[g]
        got(q2r.at[g, pl.ds(1, side - 1)], r_q2.at[g])
        qtot = q1s[g] + q2r[g, 1] + q2r[g, 2] + q2r[g, 3]
        lines = [jnp.where(lane < CAP, pltpu.roll(qtot, (LANES - CAP * i) % LANES, 1), 0.0) for i in range(per)]
        lines = pltpu.roll(jnp.concatenate(lines, axis=0), lax.rem(me, LANES // CAP) * CAP, 1)
        for i in range(per):
            qsend[START[g] + i] = lines[i : i + 1]
        for i in range(per):
            s = START[g] + i
            if s == own:
                retq[me] = qsend[s]
            else:
                rcopy(qsend.at[s], retq.at[me], s_f, r_f, far(s), mt).start()
        got(precv.at[pl.ds(1, side - 1), span(g)], r_p.at[g])
        total = pkeep[span(g)]
        for r in range(1, side):
            total = total + precv[r, span(g)].astype(F32)
        pback[pl.ds(START[g], per)] = total.astype(BF16).reshape(per, CAP, LANES)
        for i in range(per):
            s = START[g] + i
            if s == own:
                ret[me] = pback[s]
            else:
                rcopy(pback.at[s], ret.at[me], s_e, r_e, far(s), mt).start()

    def weight_grads(which):
        lhs = jnp.transpose((gsrc if which == 0 else hsrc)[...].astype(F32)).astype(BF16)
        for b in range(0, n_tp, 2):
            c = jnp.concatenate([rows[b + i, :, which].reshape(slots * CAP, LANES) for i in range(2)], axis=1)
            cols = slice(b * LANES, (b + 2) * LANES)
            if which == 0:
                r = dot(lhs, c)
                gg_out[0, :, cols] = r[:fh]
                ug_out[0, :, cols] = r[fh:]
            else:
                dg_out[0, :, cols] = dot(lhs[:fh], c)

    levels = {0: level0, 1: level1, 2: level2, 3: level3, 5: level5, 6: level6, 7: level7, 8: weight_grads, 9: weights_out}
    for k, g in PROGRAM:
        with jax.named_scope(f"L{k}g{g}"):
            levels[k](g)

    with jax.named_scope("backq"):
        got(retq.at[pl.ds(0, n_ep - 1)], r_f)
    group = LANES // CAP
    table = jnp.concatenate([jnp.sum(retq[a * group : (a + 1) * group], axis=0) for a in range(n_ep // group)], axis=1)
    table = jnp.broadcast_to(table, (8, n_ep * CAP))
    for k in range(2):
        r = dot(table, hot(k), precision=lax.Precision.HIGHEST)
        rg_out[k : k + 1, :] = r[:1] / wt[k]

    with jax.named_scope("back"):
        got(ret.at[pl.ds(0, n_ep - 1)], r_e)
    tg_out[...] = dot(pickv[...], ret[...].reshape(n_ep * CAP, LANES)).astype(BF16)

    with jax.named_scope("drain"):
        got(send.at[pl.ds(0, n_ep - 1)], s_a)
        got(rows.at[pl.ds(0, n_tp - 1)], s_b)
        got(wx.at[pl.ds(1, side - 1)], s_w)
        got(grecv.at[pl.ds(1, side - 1)], s_g)
        got(precv.at[pl.ds(1, side - 1)], s_p)
        got(q1r.at[:, pl.ds(1, side - 1)], s_q1)
        got(q2r.at[:, pl.ds(1, side - 1)], s_q2)
        got(ret.at[pl.ds(0, n_ep - 1)], s_e)
        got(retq.at[pl.ds(0, n_ep - 1)], s_f)


def write_out(n, *refs):
    copies = [pltpu.make_async_copy(refs[i], refs[n + i], refs[2 * n].at[i]) for i in range(n)]
    for c in copies:
        c.start()
    for c in copies:
        c.wait()


def per_device(nz, tokens, cotangent, expert_ids, route_weight, gate_weight, up_weight, down_weight):
    side = SIDE
    n_ep, n_tp = 2 * nz, side * side
    all_rows = n_ep * CAP
    nt = tokens.shape[0]
    fh = gate_weight.shape[1]
    vmem = pl.BlockSpec(memory_space=pltpu.VMEM)
    hbm = pl.BlockSpec(memory_space=pltpu.HBM)
    dma = pltpu.SemaphoreType.DMA
    scratch = [
        pltpu.VMEM((2, nt), jnp.int32),
        pltpu.VMEM((2, nt), BF16),
        pltpu.VMEM((nt, LANES), BF16),
        pltpu.VMEM((nt, LANES), BF16),
        pltpu.VMEM((n_tp, LANES, LANES), BF16),
        pltpu.VMEM((n_tp, LANES, LANES), BF16),
        pltpu.VMEM((n_ep, 2, CAP, LANES), BF16),
        pltpu.VMEM((n_tp, n_ep, 2, CAP, LANES), BF16),
        pltpu.VMEM((side, side, LANES, LANES), BF16),
        pltpu.VMEM((all_rows, LANES), BF16),
        pltpu.VMEM((all_rows, LANES), BF16),
        pltpu.VMEM((side, all_rows, LANES), BF16),
        pltpu.VMEM((all_rows, LANES), F32),
        pltpu.VMEM((side, all_rows, LANES), BF16),
        pltpu.VMEM((side, all_rows, LANES), BF16),
        pltpu.VMEM((n_ep, CAP, LANES), BF16),
        pltpu.VMEM((CHUNKS, 1, LANES), F32),
        pltpu.VMEM((CHUNKS, side, 1, LANES), F32),
        pltpu.VMEM((CHUNKS, 1, LANES), F32),
        pltpu.VMEM((CHUNKS, side, 1, LANES), F32),
        pltpu.VMEM((n_ep, 1, LANES), F32),
        pltpu.VMEM((n_ep, CAP, LANES), BF16),
        pltpu.VMEM((n_ep, 1, LANES), F32),
        pltpu.VMEM((nt, n_ep * CAP), BF16),
        dma((2,)), dma((2,)), dma, dma,
        dma, dma((CHUNKS,)),
        dma, dma((2 * CHUNKS * n_tp,)),
        dma, dma,
        dma, dma((CHUNKS,)),
        dma, dma((CHUNKS,)),
        dma, dma((CHUNKS,)),
        dma, dma((CHUNKS,)),
        dma, dma,
        dma, dma,
    ]
    shapes = [((nt, LANES), BF16), ((2, nt), F32)] + [(gate_weight.shape, F32)] * 3
    ins = (tokens, cotangent, expert_ids.T, route_weight.T, gate_weight, up_weight, down_weight)
    made = pl.pallas_call(
        functools.partial(kernel, nz),
        out_shape=tuple(pltpu.VMEM(*a) for a in shapes),
        in_specs=[hbm] * 7,
        out_specs=(vmem,) * 5,
        scratch_shapes=scratch,
        compiler_params=pltpu.CompilerParams(collective_id=0, has_side_effects=True, vmem_limit_bytes=24 * 1024 * 1024),
    )(*(pltpu.with_memory_space_constraint(a, pltpu.HBM) for a in ins))
    tg, rg, *grads = pl.pallas_call(
        functools.partial(write_out, 5),
        out_shape=tuple(pltpu.HBM(*a) for a in shapes),
        in_specs=[vmem] * 5,
        out_specs=(hbm,) * 5,
        scratch_shapes=[dma((5,))],
        compiler_params=pltpu.CompilerParams(vmem_limit_bytes=1024 * 1024),
    )(*(pltpu.with_memory_space_constraint(a, pltpu.VMEM) for a in made))
    return (tg, rg.T, *grads)


def solution(mesh):
    nz = mesh.shape["ep"] // 2
    in_specs = (
        P("ep", None), P("ep", None), P("ep", None), P("ep", None),
        P("ep", "tp", None), P("ep", "tp", None), P("ep", "tp", None),
    )
    out_specs = (
        P("ep", "tp"), P("ep", None), P("ep", "tp", None), P("ep", "tp", None), P("ep", "tp", None),
    )
    return jax.shard_map(
        functools.partial(per_device, nz), mesh=mesh, in_specs=in_specs, out_specs=out_specs, check_vma=False
    )
```

```python
import functools

import jax
import jax.numpy as jnp
from jax import lax
from jax.experimental import pallas as pl
from jax.experimental.pallas import tpu as pltpu
from jax.sharding import PartitionSpec as P

MESH = pl.DeviceIdType.MESH
F32, BF16 = jnp.float32, jnp.bfloat16
CAP = 16
LANES = 128
SIZES = (8, 8, 8, 8)
CHUNKS = len(SIZES)
START = tuple(sum(SIZES[:g]) for g in range(CHUNKS))
SIDE = 4


def dot(a, b, dims=((1,), (0,)), **kw):
    return lax.dot_general(a, b, (dims, ((), ())), preferred_element_type=F32, **kw)


def slot_order(nz):
    near = [0] + [d for k in range(1, nz // 2) for d in (k, nz - k)] + [nz // 2]
    n = nz // 4
    return near[:n] + near[2 * n : 3 * n] + near[n : 2 * n] + near[3 * n :]


FIRST_AXIS = (0, 1) * CHUNKS
FIRST_STEP = (1, 1, -1, -1) * CHUNKS
DIRECT1 = tuple(range(2 * CHUNKS))
XPART = (4, 5, 5, 5)
DIRECT2 = ()
WPARTS, WFIRST = 1, 1
PROGRAM = (
    (0, 0), (1, 0), (0, 1), (2, 0), (1, 1), (0, 3), (3, 0), (2, 1), (1, 3), (0, 2), (5, 0), (3, 1), (2, 3), (1, 2), (5, 1),
    (6, 0), (3, 3), (5, 3), (2, 2), (6, 1), (7, 0), (6, 3), (3, 2), (5, 2), (7, 1), (8, 0), (7, 3), (6, 2), (8, 1), (7, 2),
)


def kernel(nz, tok, cot, ids_hbm, rw_hbm, gw, uw, dw, tg_out, rg_out, gg_out, ug_out, dg_out,
           ids_ref, rw_ref, tokc, cotc, wgu, wd, send, rows, wx, gsrc, hsrc, grecv, pkeep, psrc, precv,
           pback, q0, q1r, q1s, q2r, qsend, ret, retq, pickv,
           sem_i, sem_tc, sem_w, sem_wd, s_a, r_a, s_b, r_b, s_w, r_w, s_g, r_g, s_p, r_p,
           s_q1, r_q1, s_q2, r_q2, s_e, r_e, s_f, r_f):
    side = SIDE
    n_ep, n_tp = 2 * nz, side * side
    order = slot_order(nz)
    slots = n_ep
    own = 2 * order.index(0)
    assert own in START and sum(SIZES) == slots
    me, mt = lax.axis_index("ep"), lax.axis_index("tp")
    z, core = me // 2, lax.rem(me, 2)
    y, x = mt // side, lax.rem(mt, side)
    fh = gw.shape[1]
    nt = tokc.shape[0]

    col = pl.ds(pl.multiple_of(mt * LANES, LANES), LANES)
    load_i = pltpu.make_async_copy(ids_hbm, ids_ref, sem_i.at[0])
    load_r = pltpu.make_async_copy(rw_hbm, rw_ref, sem_i.at[1])
    load_t = pltpu.make_async_copy(tok.at[:, col], tokc, sem_tc.at[0])
    load_c = pltpu.make_async_copy(cot.at[:, col], cotc, sem_tc.at[1])
    for load in (load_i, load_r, load_t, load_c):
        load.start()

    def at(dx, dy):
        return lax.rem(y + dy, side) * side + lax.rem(x + dx, side)

    def along(axis, d):
        return at(d, 0) if axis == 0 else at(0, d)

    def far(slot):
        return lax.rem(z + order[slot // 2], nz) * 2 + lax.rem(core + slot % 2, 2)

    def back_slot(slot):
        return 2 * order.index((nz - order[slot // 2]) % nz) + slot % 2

    def rcopy(src, dst, ssem, rsem, ep, tp):
        return pltpu.make_async_remote_copy(
            src_ref=src, dst_ref=dst, send_sem=ssem, recv_sem=rsem,
            device_id={"ep": ep, "tp": tp}, device_id_type=MESH,
        )

    def got(ref, rsem):
        pltpu.make_async_copy(ref, ref, rsem).wait()

    barrier = pltpu.get_barrier_semaphore()

    def greet(i, carry):
        pl.semaphore_signal(barrier, inc=1, device_id={"ep": lax.rem(me + i, n_ep), "tp": mt}, device_id_type=MESH)
        return carry

    lax.fori_loop(1, n_ep, greet, 0)
    for d in range(1, side):
        for axis in range(2):
            pl.semaphore_signal(barrier, inc=1, device_id={"ep": me, "tp": along(axis, d)}, device_id_type=MESH)

    for b in range(n_tp):
        cols = pl.ds(b * LANES, LANES)
        pltpu.make_async_copy(gw.at[0, :, cols], wgu.at[b, pl.ds(0, fh)], sem_w).start()
        pltpu.make_async_copy(uw.at[0, :, cols], wgu.at[b, pl.ds(fh, fh)], sem_w).start()

    load_i.wait()
    load_r.wait()
    ids = [ids_ref[k : k + 1, :] for k in range(2)]
    wt = [rw_ref[k : k + 1, :].astype(F32) for k in range(2)]
    e_row = lax.broadcasted_iota(jnp.int32, (n_ep, nt), 0)
    mem = [(e_row == ids[k]).astype(F32) for k in range(2)]
    upper = (lax.broadcasted_iota(jnp.int32, (nt, nt), 0) < lax.broadcasted_iota(jnp.int32, (nt, nt), 1)).astype(BF16)
    before = dot((mem[0] + mem[1]).astype(BF16), upper)
    rank = [jnp.sum(mem[k] * before, axis=0, keepdims=True).astype(jnp.int32) for k in range(2)]
    place_of = [ids[k] * CAP + rank[k] for k in range(2)]

    def hot(k):
        return (lax.broadcasted_iota(jnp.int32, (n_ep * CAP, nt), 0) == place_of[k]).astype(F32)

    h0, h1 = hot(0), hot(1)
    pick_t = h0 + h1
    scaled_t = h0 * wt[0] + h1 * wt[1]
    load_t.wait()
    load_c.wait()
    send[:, 0] = dot(pick_t.astype(BF16), tokc[...]).astype(BF16).reshape(n_ep, CAP, LANES)
    send[:, 1] = dot(scaled_t.astype(BF16), cotc[...]).astype(BF16).reshape(n_ep, CAP, LANES)
    rows[mt, own] = send[me]
    got(wgu, sem_w)

    with jax.named_scope("bar"):
        pl.semaphore_wait(barrier, n_ep - 1 + 2 * (side - 1))

    def dispatch(chunk):
        for s in range(START[chunk], START[chunk] + SIZES[chunk]):
            if s != own:
                e = far(back_slot(s))
                rcopy(send.at[e], rows.at[mt, s], s_a, r_a.at[chunk], e, mt).start()

    dispatch(0)

    def weights_out(part):
        w4 = wgu.reshape(side, side, LANES, LANES)
        some = pl.ds(part * side // WPARTS, side // WPARTS)
        for d in range(1, side):
            rcopy(w4.at[some, lax.rem(x + d, side)], wx.at[side - d, some], s_w, r_w, me, along(0, d)).start()

    for part in range(WFIRST):
        weights_out(part)
    for b in range(n_tp):
        cols = pl.ds(b * LANES, LANES)
        for h in range(2):
            pltpu.make_async_copy(dw.at[0, :, cols], wd.at[b, pl.ds(h * fh, fh)], sem_wd).start()
    pickv[...] = jnp.transpose(pick_t).astype(BF16)
    got(wd, sem_wd)
    for chunk in (1, 3, 2):
        dispatch(chunk)

    def ref_of(q, du, dv):
        b = at(du, dv) if FIRST_AXIS[q] == 0 else at(dv, du)
        g = q // 2
        n = XPART[g]
        return rows.at[b, pl.ds(START[g] + n, SIZES[g] - n) if q % 2 else pl.ds(START[g], n)]

    def span(g):
        return pl.ds(START[g] * CAP, SIZES[g] * CAP)

    def pass_on(q, du, dv, second, step):
        rdu, rdv = (du, (dv - step) % side) if second else ((du - step) % side, dv)
        axis = FIRST_AXIS[q] ^ int(second)
        ref = ref_of(q, du, dv)
        rcopy(ref, ref, s_b, r_b.at[(q * side + rdu) * side + rdv], me, along(axis, step % side)).start()

    def block(q, du, dv):
        got(ref_of(q, du, dv), r_b.at[(q * side + du) * side + dv])

    def both(q, du, dv, second):
        pass_on(q, du, dv, second, 1)
        pass_on(q, du, dv, second, -1)

    def relay(q, keep, second):
        step = FIRST_STEP[q] if not second else 1 if (q + keep) % 2 == 0 else -1
        v = side - 1 if step == 1 else 1
        pass_on(q, *((keep, v) if second else (v, keep)), second, step)

    def spread(q, du):
        both(q, du, 0, True)
        if q in DIRECT2:
            pass_on(q, du, 0, True, 2)

    def halves(g):
        return (2 * g, 2 * g + 1)

    def level0(g):
        skip = 1 if START[g] == own else 0
        got(rows.at[mt, pl.ds(START[g] + skip, SIZES[g] - skip)], r_a.at[g])
        for q in halves(g):
            both(q, 0, 0, False)
            if q in DIRECT1:
                pass_on(q, 0, 0, False, 2)
        for q in halves(g):
            spread(q, 0)

    def second_in(q, du):
        if q not in DIRECT2:
            block(q, du, 1)
            block(q, du, side - 1)
            relay(q, du, True)

    def level1(g):
        for q in reversed(halves(g)) if g == 0 else halves(g):
            for du in (1, side - 1):
                block(q, du, 0)
                spread(q, du)
            if q not in DIRECT1:
                relay(q, 0, False)
        for q in halves(g):
            block(q, 2, 0)
            spread(q, 2)

    def level2(g):
        for du in (0, 1, side - 1, 2):
            for q in halves(g):
                second_in(q, du)

    def level3(g):
        for q in halves(g):
            for du in range(side):
                if q in DIRECT2:
                    block(q, du, 1)
                    block(q, du, side - 1)
                block(q, du, 2)

    def level5(g):
        per = SIZES[g]
        crows = per * CAP
        half = lax.broadcasted_iota(jnp.int32, (crows, LANES), 1) < fh
        pre = jnp.zeros((crows, LANES), F32)
        back = jnp.zeros((crows, LANES), F32)
        for b in range(0, n_tp, 2):
            a = [rows[b + i, pl.ds(START[g], per)] for i in range(2)]
            t = jnp.concatenate([a[i][:, 0].reshape(crows, LANES) for i in range(2)], axis=1)
            c = jnp.concatenate([a[i][:, 1].reshape(crows, LANES) for i in range(2)], axis=1)
            wt_b = jnp.concatenate([wgu[b], wgu[b + 1]], axis=1)
            wd_b = jnp.concatenate([wd[b], wd[b + 1]], axis=1)
            pre = pre + dot(t, wt_b, ((1,), (1,)))
            back = back + dot(c, wd_b, ((1,), (1,)))
        other = pltpu.roll(pre, fh, 1)
        gate = jnp.where(half, pre, other)
        up = jnp.where(half, other, pre)
        sig = jax.nn.sigmoid(gate)
        silu = gate * sig
        hidden = silu * up
        grad = back * jnp.where(half, up * sig * (1.0 + gate * (1.0 - sig)), silu)
        gsrc[span(g)] = grad.astype(BF16)
        hsrc[span(g)] = hidden.astype(BF16)
        prod = jnp.where(half, hidden * back, 0.0)
        if crows < LANES:
            prod = jnp.concatenate([prod, jnp.zeros((LANES - crows, LANES), F32)], axis=0)
        prod = jnp.transpose(prod)
        q0[g] = jnp.sum(prod, axis=0, keepdims=True)
        for d in range(1, side):
            rcopy(gsrc.at[span(g)], grecv.at[side - d, span(g)], s_g, r_g.at[g], me, along(0, d)).start()
        for d in range(1, side):
            rcopy(q0.at[g], q1r.at[g, side - d], s_q1, r_q1.at[g], me, along(0, d)).start()

    def level6(g):
        if g == 0:
            got(wx.at[pl.ds(1, side - 1)], r_w)
        crows = SIZES[g] * CAP
        got(q1r.at[g, pl.ds(1, side - 1)], r_q1.at[g])
        q1s[g] = q0[g] + q1r[g, 1] + q1r[g, 2] + q1r[g, 3]
        for d in range(1, side):
            rcopy(q1s.at[g], q2r.at[g, side - d], s_q2, r_q2.at[g], me, along(1, d)).start()
        got(grecv.at[pl.ds(1, side - 1), span(g)], r_g.at[g])
        lhs = [gsrc[span(g)]] + [grecv[r, span(g)] for r in range(1, side)]
        lhs = [jnp.concatenate(lhs[k : k + 2], axis=1) for k in range(0, side, 2)]
        for d in reversed(range(0, side, 2)):
            acc = jnp.zeros((crows, 2 * LANES), F32)
            for k in range(0, side, 2):
                parts = []
                for r in (k, k + 1):
                    w = []
                    for dd in (d, d + 1):
                        w.append(wgu[along(1, dd)] if r == 0 else wx[r, lax.rem(y + dd, side)])
                    parts.append(jnp.concatenate(w, axis=1))
                acc = acc + dot(lhs[k // 2], jnp.concatenate(parts, axis=0))
            for i, dd in enumerate((d, d + 1)):
                piece = acc[:, i * LANES : (i + 1) * LANES]
                if dd == 0:
                    pkeep[span(g)] = piece
                else:
                    psrc[dd, span(g)] = piece.astype(BF16)
        for d in range(1, side):
            rcopy(psrc.at[d, span(g)], precv.at[side - d, span(g)], s_p, r_p.at[g], me, along(1, d)).start()

    lane = lax.broadcasted_iota(jnp.int32, (1, LANES), 1)

    def level7(g):
        per = SIZES[g]
        got(q2r.at[g, pl.ds(1, side - 1)], r_q2.at[g])
        qtot = q1s[g] + q2r[g, 1] + q2r[g, 2] + q2r[g, 3]
        lines = [jnp.where(lane < CAP, pltpu.roll(qtot, (LANES - CAP * i) % LANES, 1), 0.0) for i in range(per)]
        lines = pltpu.roll(jnp.concatenate(lines, axis=0), lax.rem(me, LANES // CAP) * CAP, 1)
        for i in range(per):
            qsend[START[g] + i] = lines[i : i + 1]
        for i in range(per):
            s = START[g] + i
            if s == own:
                retq[me] = qsend[s]
            else:
                rcopy(qsend.at[s], retq.at[me], s_f, r_f, far(s), mt).start()
        got(precv.at[pl.ds(1, side - 1), span(g)], r_p.at[g])
        total = pkeep[span(g)]
        for r in range(1, side):
            total = total + precv[r, span(g)].astype(F32)
        pback[pl.ds(START[g], per)] = total.astype(BF16).reshape(per, CAP, LANES)
        for i in range(per):
            s = START[g] + i
            if s == own:
                ret[me] = pback[s]
            else:
                rcopy(pback.at[s], ret.at[me], s_e, r_e, far(s), mt).start()

    def weight_grads(which):
        lhs = jnp.transpose((gsrc if which == 0 else hsrc)[...].astype(F32)).astype(BF16)
        for b in range(0, n_tp, 2):
            c = jnp.concatenate([rows[b + i, :, which].reshape(slots * CAP, LANES) for i in range(2)], axis=1)
            cols = slice(b * LANES, (b + 2) * LANES)
            if which == 0:
                r = dot(lhs, c)
                gg_out[0, :, cols] = r[:fh]
                ug_out[0, :, cols] = r[fh:]
            else:
                dg_out[0, :, cols] = dot(lhs[:fh], c)

    levels = {0: level0, 1: level1, 2: level2, 3: level3, 5: level5, 6: level6, 7: level7, 8: weight_grads, 9: weights_out}
    for k, g in PROGRAM:
        with jax.named_scope(f"L{k}g{g}"):
            levels[k](g)

    with jax.named_scope("backq"):
        got(retq.at[pl.ds(0, n_ep - 1)], r_f)
    group = LANES // CAP
    table = jnp.concatenate([jnp.sum(retq[a * group : (a + 1) * group], axis=0) for a in range(n_ep // group)], axis=1)
    table = jnp.broadcast_to(table, (8, n_ep * CAP))
    for k in range(2):
        r = dot(table, hot(k), precision=lax.Precision.HIGHEST)
        rg_out[k : k + 1, :] = r[:1] / wt[k]

    with jax.named_scope("back"):
        got(ret.at[pl.ds(0, n_ep - 1)], r_e)
    tg_out[...] = dot(pickv[...], ret[...].reshape(n_ep * CAP, LANES)).astype(BF16)

    with jax.named_scope("drain"):
        got(send.at[pl.ds(0, n_ep - 1)], s_a)
        got(rows.at[pl.ds(0, n_tp - 1)], s_b)
        got(wx.at[pl.ds(1, side - 1)], s_w)
        got(grecv.at[pl.ds(1, side - 1)], s_g)
        got(precv.at[pl.ds(1, side - 1)], s_p)
        got(q1r.at[:, pl.ds(1, side - 1)], s_q1)
        got(q2r.at[:, pl.ds(1, side - 1)], s_q2)
        got(ret.at[pl.ds(0, n_ep - 1)], s_e)
        got(retq.at[pl.ds(0, n_ep - 1)], s_f)


def write_out(n, *refs):
    copies = [pltpu.make_async_copy(refs[i], refs[n + i], refs[2 * n].at[i]) for i in range(n)]
    for c in copies:
        c.start()
    for c in copies:
        c.wait()


def per_device(nz, tokens, cotangent, expert_ids, route_weight, gate_weight, up_weight, down_weight):
    side = SIDE
    n_ep, n_tp = 2 * nz, side * side
    all_rows = n_ep * CAP
    nt = tokens.shape[0]
    fh = gate_weight.shape[1]
    vmem = pl.BlockSpec(memory_space=pltpu.VMEM)
    hbm = pl.BlockSpec(memory_space=pltpu.HBM)
    dma = pltpu.SemaphoreType.DMA
    scratch = [
        pltpu.VMEM((2, nt), jnp.int32),
        pltpu.VMEM((2, nt), BF16),
        pltpu.VMEM((nt, LANES), BF16),
        pltpu.VMEM((nt, LANES), BF16),
        pltpu.VMEM((n_tp, LANES, LANES), BF16),
        pltpu.VMEM((n_tp, LANES, LANES), BF16),
        pltpu.VMEM((n_ep, 2, CAP, LANES), BF16),
        pltpu.VMEM((n_tp, n_ep, 2, CAP, LANES), BF16),
        pltpu.VMEM((side, side, LANES, LANES), BF16),
        pltpu.VMEM((all_rows, LANES), BF16),
        pltpu.VMEM((all_rows, LANES), BF16),
        pltpu.VMEM((side, all_rows, LANES), BF16),
        pltpu.VMEM((all_rows, LANES), F32),
        pltpu.VMEM((side, all_rows, LANES), BF16),
        pltpu.VMEM((side, all_rows, LANES), BF16),
        pltpu.VMEM((n_ep, CAP, LANES), BF16),
        pltpu.VMEM((CHUNKS, 1, LANES), F32),
        pltpu.VMEM((CHUNKS, side, 1, LANES), F32),
        pltpu.VMEM((CHUNKS, 1, LANES), F32),
        pltpu.VMEM((CHUNKS, side, 1, LANES), F32),
        pltpu.VMEM((n_ep, 1, LANES), F32),
        pltpu.VMEM((n_ep, CAP, LANES), BF16),
        pltpu.VMEM((n_ep, 1, LANES), F32),
        pltpu.VMEM((nt, n_ep * CAP), BF16),
        dma((2,)), dma((2,)), dma, dma,
        dma, dma((CHUNKS,)),
        dma, dma((2 * CHUNKS * n_tp,)),
        dma, dma,
        dma, dma((CHUNKS,)),
        dma, dma((CHUNKS,)),
        dma, dma((CHUNKS,)),
        dma, dma((CHUNKS,)),
        dma, dma,
        dma, dma,
    ]
    shapes = [((nt, LANES), BF16), ((2, nt), F32)] + [(gate_weight.shape, F32)] * 3
    ins = (tokens, cotangent, expert_ids.T, route_weight.T, gate_weight, up_weight, down_weight)
    made = pl.pallas_call(
        functools.partial(kernel, nz),
        out_shape=tuple(pltpu.VMEM(*a) for a in shapes),
        in_specs=[hbm] * 7,
        out_specs=(vmem,) * 5,
        scratch_shapes=scratch,
        compiler_params=pltpu.CompilerParams(collective_id=0, has_side_effects=True, vmem_limit_bytes=24 * 1024 * 1024),
    )(*(pltpu.with_memory_space_constraint(a, pltpu.HBM) for a in ins))
    tg, rg, *grads = pl.pallas_call(
        functools.partial(write_out, 5),
        out_shape=tuple(pltpu.HBM(*a) for a in shapes),
        in_specs=[vmem] * 5,
        out_specs=(hbm,) * 5,
        scratch_shapes=[dma((5,))],
        compiler_params=pltpu.CompilerParams(vmem_limit_bytes=1024 * 1024),
    )(*(pltpu.with_memory_space_constraint(a, pltpu.VMEM) for a in made))
    return (tg, rg.T, *grads)


def solution(mesh):
    nz = mesh.shape["ep"] // 2
    in_specs = (
        P("ep", None), P("ep", None), P("ep", None), P("ep", None),
        P("ep", "tp", None), P("ep", "tp", None), P("ep", "tp", None),
    )
    out_specs = (
        P("ep", "tp"), P("ep", None), P("ep", "tp", None), P("ep", "tp", None), P("ep", "tp", None),
    )
    return jax.shard_map(
        functools.partial(per_device, nz), mesh=mesh, in_specs=in_specs, out_specs=out_specs, check_vma=False
    )
```
